512 devices in a mesh: grp: 2 (over y), dp: 8 (over x), kv: 16 (over z), tp: 2 (over core).
Axes of the slice: x: 8, y: 2, z: 16, core: 2. Of those that a mesh axis runs over, the one named last changes fastest.
The devices are a block of a 8x8x16 slice.
Arguments:
- candidate_vectors: bfloat16 [512, 4, 2048], P(('grp', 'dp'), None, ('kv', 'tp')), parts along dimension 0, may hold values from -6 to 6
- leading_scaling_factor: bfloat16 [2048], replicated, may hold values from 0.099609375 to 1.8984375
- lane_feed_matrix: bfloat16 [2048, 32, 2, 64], P(None, 'kv', 'tp')
- final_valve_matrix: bfloat16 [2048, 32, 2, 64], P(None, 'kv', 'tp'), may hold values from -0.125 to 0.125
- increment_matrix: bfloat16 [2048, 32, 2], replicated, may hold values from -0.125 to 0.125
- entry_basis_matrix: bfloat16 [2048, 2, 128], P(None, 'tp'), may hold values from -0.125 to 0.125
- readout_basis_matrix: bfloat16 [2048, 2, 128], P(None, 'tp'), may hold values from -0.125 to 0.125
- lane_feed_kernel: float32 [4, 32, 2, 64], P(None, 'kv', 'tp'), may hold values from -3 to 3
- entry_basis_kernel: float32 [4, 2, 128], P(None, 'tp'), may hold values from -3 to 3
- readout_basis_kernel: float32 [4, 2, 128], P(None, 'tp'), may hold values from -3 to 3
- increment_offset: float32 [32, 2], P('kv', 'tp'), may hold values from -4 to 1
- shrink_speed_exponent: float32 [32, 2], P('kv', 'tp'), may hold values from 0 to 2.8
- lane_bypass_factor: float32 [32, 2], P('kv', 'tp'), may hold values from 0.5 to 1.5
- final_linear_matrix: bfloat16 [32, 2, 64, 2048], P(None, None, None, ('kv', 'tp')), may hold values from -0.09375 to 0.09375
- hidden_carried_memory: float32 [512, 32, 2, 64, 128], P(('grp', 'dp'), 'kv', 'tp'), parts along dimension 0, may hold values from -0.6 to 0.6
- lane_filter_memory: bfloat16 [512, 7, 32, 2, 64], P(('grp', 'dp'), None, 'kv', 'tp'), parts along dimension 0, may hold values from -6 to 6
- entry_basis_memory: bfloat16 [512, 7, 2, 128], P(('grp', 'dp'), None, 'tp'), parts along dimension 0, may hold values from -6 to 6
- readout_basis_memory: bfloat16 [512, 7, 2, 128], P(('grp', 'dp'), None, 'tp'), parts along dimension 0, may hold values from -6 to 6
- predecessor_index: int32 [512, 4], P(('grp', 'dp')), parts along dimension 0, may hold values from -1 to 2, as said below
- admitted_counts: int32 [512], P(('grp', 'dp')), parts along dimension 0, may hold values from 0 to 4
- surplus_fading: float32 [512, 4, 32, 2], P(('grp', 'dp'), None, 'kv', 'tp'), parts along dimension 0, may hold values from -0.7 to 0, as said below
Outputs:
- mixed: bfloat16 [512, 4, 2048], P(('grp', 'dp'), None, ('kv', 'tp')), parts along dimension 0
The draws below stay inside these ranges and needn't reach their ends.
There are 2 independent parts, one for each index of `grp`. The reference program is written for one: setup_inputs(seed, part) draws one part's arguments, and reference() takes and returns one part's arrays. A program takes and returns all parts, laid end to end along the dimension named above; an argument that names none is the same for every part. Nothing has to cross between parts.
Inputs may be any that keep to these rules, and one draw needn't show every extreme that they name: predecessor_index[s, j] is -1 or a smaller proposal index than j. `surplus_fading`: zero except at a few proposals and heads.
All inputs are finite; a program needn't handle non-finite values.
Results may differ from the reference program's by a relative error of at most 0.012.
Values may be sent and summed in bfloat16 or wider, within the bound.
No kernel may reach another device: no remote copies, remote signals or barrier semaphores. Data moves between devices by JAX's collectives and lax.ppermute only.
A program may use at most 64 MiB of HBM per device.

```python
import jax
import jax.numpy as jnp
from jax import lax

D = 2048
HG = 32
G = 2
HD = 64
N = 128
CONV = 4
PROP = 4
PREV = 4
WIN = 7
SEQS = 256


def draw_lane_feed_matrix(key, part):
    first, second = jax.random.split(key)
    base = jax.random.normal(first, (D, HG, G, HD), jnp.float32) * D ** (-0.5)
    order = (jnp.arange(HG)[:, None] * G + jnp.arange(G)[None, :]).astype(jnp.float32) / (HG * G - 1)
    spread = 3.0
    scale = spread ** (order - 0.5)
    jitter = jax.random.uniform(second, (HG, G, HD), jnp.float32, 0.7, 1.4)
    return (base * scale[None, :, :, None] * jitter[None]).astype(jnp.bfloat16)


def draw_predecessor_index(key, part):
    upper = jnp.arange(PROP, dtype=jnp.int32)[None, :]
    return jax.random.randint(key, (SEQS, PROP), -1, upper).astype(jnp.int32)


def draw_surplus_fading(key, part):
    first, second = jax.random.split(jax.random.fold_in(key, 7))
    struck = jax.random.uniform(first, (SEQS, PROP, HG, G), jnp.float32) < 0.15
    amount = jax.random.uniform(second, (SEQS, PROP, HG, G), jnp.float32, -0.7, -0.22)
    return jnp.where(struck, amount, 0.0)


def place_ends(array, key, low, top_value):
    longest = array.shape.index(max(array.shape))
    spots = []
    for shift in (0, 1):
        where = [jax.random.randint(jax.random.fold_in(key, axis), (), 0, length) for axis, length in enumerate(array.shape)]
        where[longest] = (where[longest] + shift) % array.shape[longest]
        spots.append(tuple(where))
    return array.at[spots[0]].set(low).at[spots[1]].set(top_value)


def steps_of(rng, extent, shards, smallest, largest):
    def one(dim, shards_of):
        steps = jax.random.uniform(jax.random.fold_in(jax.random.fold_in(rng, 6), dim), (shards_of,), jnp.float32, smallest / len(shards), largest / len(shards))
        return jnp.repeat(jnp.exp(steps), extent[dim] // shards_of).reshape((-1,) + (1,) * (len(extent) - dim - 1))

    factor_of = one(*shards[0])
    for cut in shards[1:]:
        factor_of = factor_of * one(*cut)
    return factor_of


def gaussian(stream_key, shape, scale, limit, cuts=(), kind=jnp.bfloat16):
    result = scale * jax.random.normal(stream_key, shape, jnp.float32)
    if cuts:
        result = result * steps_of(stream_key, shape, cuts, -0.22, 0.18)
    return jnp.clip(result, -limit, limit).astype(kind)


def setup_inputs(seed: int = 0, part: int = 0) -> dict:
    key_of = jax.random.split(jax.random.key(seed), 22)
    part_splits = jax.random.split(jax.random.fold_in(key_of[21], part), 22)
    return {
        "candidate_vectors": gaussian(part_splits[0], (SEQS, PROP, D), 1.0, 6.0, ((0, 8), (2, 32))),
        "leading_scaling_factor": jnp.clip(1.0 + 0.18 * jax.random.normal(key_of[1], (D,), jnp.float32), 0.099609375, 1.8984375).astype(jnp.bfloat16),
        "lane_feed_matrix": draw_lane_feed_matrix(jax.random.fold_in(key_of[21], 71), part),
        "final_valve_matrix": gaussian(key_of[3], (D, HG, G, HD), D ** -0.5, 0.125, ((1, 16), (2, 2))),
        "increment_matrix": gaussian(key_of[4], (D, HG, G), D ** -0.5, 0.125),
        "entry_basis_matrix": gaussian(key_of[5], (D, G, N), D ** -0.5, 0.125, ((1, 2),)),
        "readout_basis_matrix": gaussian(key_of[6], (D, G, N), D ** -0.5, 0.125, ((1, 2),)),
        "lane_feed_kernel": gaussian(key_of[7], (CONV, HG, G, HD), 0.5, 3.0, ((1, 16), (2, 2)), jnp.float32),
        "entry_basis_kernel": gaussian(key_of[8], (CONV, G, N), 0.5, 3.0, ((1, 2),), jnp.float32),
        "readout_basis_kernel": gaussian(key_of[9], (CONV, G, N), 0.5, 3.0, ((1, 2),), jnp.float32),
        "increment_offset": jnp.clip(-4.0 + 5.0 * jax.random.uniform(key_of[10], (HG, G), jnp.float32) ** steps_of(key_of[10], (HG, G), ((0, 16), (1, 2)), -0.2, 0.2), -4.0, 1.0),
        "shrink_speed_exponent": jnp.clip(2.8 * jax.random.uniform(key_of[11], (HG, G), jnp.float32) ** steps_of(key_of[11], (HG, G), ((0, 16), (1, 2)), -0.2, 0.2), 0.0, 2.8),
        "lane_bypass_factor": jnp.clip(0.5 + 1.0 * jax.random.uniform(key_of[12], (HG, G), jnp.float32) ** steps_of(key_of[12], (HG, G), ((0, 16), (1, 2)), -0.2, 0.2), 0.5, 1.5),
        "final_linear_matrix": gaussian(key_of[13], (HG, G, HD, D), (HG * G * HD) ** -0.5, 0.09375, ((3, 32),)),
        "hidden_carried_memory": gaussian(part_splits[14], (SEQS, HG, G, HD, N), 0.1, 0.6, ((0, 8), (1, 16), (2, 2)), jnp.float32),
        "lane_filter_memory": gaussian(part_splits[15], (SEQS, WIN, HG, G, HD), 1.0, 6.0, ((0, 8), (2, 16), (3, 2))),
        "entry_basis_memory": gaussian(part_splits[16], (SEQS, WIN, G, N), 1.0, 6.0, ((0, 8), (2, 2))),
        "readout_basis_memory": gaussian(part_splits[17], (SEQS, WIN, G, N), 1.0, 6.0, ((0, 8), (2, 2))),
        "predecessor_index": draw_predecessor_index(jax.random.fold_in(jax.random.fold_in(key_of[21], part), 71), part),
        "admitted_counts": place_ends(jax.random.randint(part_splits[19], (SEQS,), 0, PREV + 1), jax.random.fold_in(part_splits[19], 1), 0, PREV).astype(jnp.int32),
        "surplus_fading": draw_surplus_fading(jax.random.fold_in(jax.random.fold_in(key_of[21], part), 71), part),
    }


HIGH = lax.Precision.HIGHEST

def lineage_tables(predecessor_index):
    seqs, props = predecessor_index.shape
    column = jnp.arange(props, dtype=jnp.int32)
    current = jnp.broadcast_to(column[None, :], (seqs, props)).astype(jnp.int32)
    depth = jnp.zeros((seqs, props), jnp.int32)
    onehots = []
    for step in range(props):
        onehots.append((current[:, :, None] == column[None, None, :]).astype(jnp.float32))
        if step > 0:
            depth = depth + (current >= 0).astype(jnp.int32)
        upward = jnp.take_along_axis(predecessor_index, jnp.maximum(current, 0).astype(jnp.int32), axis=1)
        current = jnp.where(current >= 0, upward, -1).astype(jnp.int32)
    return (onehots, depth)

def conv_tree(current, saved, taps, onehots, depth, admitted_counts):
    props = current.shape[1]
    slots = jnp.arange(saved.shape[1], dtype=jnp.int32)
    cur_f = current.astype(jnp.float32)
    saved_f = saved.astype(jnp.float32)
    total = jnp.zeros(cur_f.shape, jnp.float32)
    for lag in range(CONV):
        value = jnp.zeros(cur_f.shape, jnp.float32)
        if lag < props:
            value = jnp.einsum('sji,sic->sjc', onehots[lag], cur_f, precision=HIGH)
        target = (admitted_counts[:, None] + (CONV - 1) - (lag - depth)).astype(jnp.int32)
        chosen = ((depth < lag)[:, :, None] & (slots[None, None, :] == target[:, :, None])).astype(jnp.float32)
        value = value + jnp.einsum('sjw,swc->sjc', chosen, saved_f, precision=HIGH)
        total = total + taps[CONV - 1 - lag].astype(jnp.float32) * value
    return jax.nn.silu(total)

def reference(candidate_vectors, leading_scaling_factor, lane_feed_matrix, final_valve_matrix, increment_matrix, entry_basis_matrix, readout_basis_matrix, lane_feed_kernel, entry_basis_kernel, readout_basis_kernel, increment_offset, shrink_speed_exponent, lane_bypass_factor, final_linear_matrix, hidden_carried_memory, lane_filter_memory, entry_basis_memory, readout_basis_memory, predecessor_index, admitted_counts, surplus_fading):
    seqs, props, _ = candidate_vectors.shape
    tok_f = candidate_vectors.astype(jnp.float32)
    r_in = lax.rsqrt(lax.optimization_barrier(jnp.mean(tok_f * tok_f, axis=-1)) + 1e-06).reshape(seqs * props, 1)
    scaled = (tok_f * leading_scaling_factor.astype(jnp.float32)).astype(jnp.bfloat16).reshape(seqs * props, D)

    def project(weight):
        return jnp.dot(scaled, weight.reshape(D, -1), preferred_element_type=jnp.float32) * r_in
    x_rows = project(lane_feed_matrix).astype(jnp.bfloat16).reshape(seqs, props, HG * G * HD)
    z_rows = project(final_valve_matrix).astype(jnp.bfloat16).reshape(seqs, props, HG, G, HD)
    dt_raw = project(increment_matrix).reshape(seqs, props, HG, G)
    b_rows = project(entry_basis_matrix).astype(jnp.bfloat16).reshape(seqs, props, G * N)
    c_rows = project(readout_basis_matrix).astype(jnp.bfloat16).reshape(seqs, props, G * N)
    onehots, depth = lineage_tables(predecessor_index)
    x_conv = conv_tree(x_rows, lane_filter_memory.reshape(seqs, WIN, -1), lane_feed_kernel.reshape(CONV, -1), onehots, depth, admitted_counts).reshape(seqs, props, HG, G, HD)
    b_conv = conv_tree(b_rows, entry_basis_memory.reshape(seqs, WIN, -1), entry_basis_kernel.reshape(CONV, -1), onehots, depth, admitted_counts).reshape(seqs, props, G, N)
    c_conv = conv_tree(c_rows, readout_basis_memory.reshape(seqs, WIN, -1), readout_basis_kernel.reshape(CONV, -1), onehots, depth, admitted_counts).reshape(seqs, props, G, N)
    lineage = sum(onehots)
    lane_increment = jax.nn.softplus(dt_raw + increment_offset)
    fading_exponent = -jnp.exp(shrink_speed_exponent) * lane_increment + surplus_fading
    level = jnp.einsum('sji,sihg->sjhg', lineage, fading_exponent, precision=HIGH)
    gap = level[:, :, None] - level[:, None, :]
    weight = jnp.where(lineage[:, :, :, None, None] > 0, jnp.exp(jnp.minimum(gap, 0.0)), 0.0)
    scores = jnp.einsum('sjgn,sign->sjig', c_conv, b_conv, precision=HIGH)
    mixing = weight * scores[:, :, :, None, :] * lane_increment[:, None]
    y_rows = jnp.einsum('sjihg,sihgp->sjhgp', mixing, x_conv, precision=HIGH)
    y_rows = y_rows + jnp.exp(level)[..., None] * jnp.einsum('shgpn,sjgn->sjhgp', hidden_carried_memory, c_conv, precision=HIGH)
    y_rows = y_rows + lane_bypass_factor[..., None] * x_conv
    gated = (y_rows * jax.nn.silu(z_rows.astype(jnp.float32))).astype(jnp.bfloat16).reshape(seqs * props, -1)
    gated_f = gated.astype(jnp.float32)
    r_out = lax.rsqrt(lax.optimization_barrier(jnp.mean(gated_f * gated_f, axis=-1)) + 1e-05)
    mixed = jnp.dot(gated, final_linear_matrix.reshape(-1, D), preferred_element_type=jnp.float32) * r_out[:, None]
    return mixed.astype(jnp.bfloat16).reshape(seqs, props, D)
```

```python
import functools

import jax
import jax.numpy as jnp
from jax import lax
from jax.experimental import pallas as pl
from jax.experimental.pallas import tpu as pltpu
from jax.sharding import PartitionSpec as P

D = 2048
HG = 32
G = 2
HD = 64
N = 128
CONV = 4
WIN = 7
PROP = 4
PREV = 4

INTERPRET = False


def vmem(count):
    return [pl.BlockSpec(memory_space=pltpu.VMEM)] * count


def silu(x):
    return x / (1.0 + jnp.exp(-x))


def pack_kernel(rows_ref, out_ref, wide):
    seqs = rows_ref.shape[0]
    for j in range(PROP):
        wide[j] = rows_ref[:, j, :].astype(jnp.float32)
    packed = jnp.concatenate(
        [
            jnp.concatenate([wide[0], wide[1]], axis=0),
            jnp.concatenate([wide[2], wide[3]], axis=0),
        ],
        axis=1,
    ).astype(jnp.bfloat16)
    for copy in range(out_ref.shape[0]):
        out_ref[copy] = packed


def mixer_kernel(
    pieces_ref,
    gain_ref,
    wx_ref,
    wz_ref,
    wdt_ref,
    wb_ref,
    wc_ref,
    taps_ref,
    heads_ref,
    state_ref,
    mem_x_ref,
    mem_b_ref,
    mem_c_ref,
    table_ref,
    fading_ref,
    out_ref,
    cc_all,
    read_all,
):
    half = pieces_ref.shape[2]
    seqs = half // 2
    rows = 2 * half
    kv_count = pieces_ref.shape[1]
    f32 = jnp.float32
    lane = lax.broadcasted_iota(jnp.int32, (half, 2 * HD), 1)
    left = lane < HD
    scaled = []
    square = jnp.zeros((rows, 2 * HD), f32)
    for k in range(kv_count):
        p0 = pieces_ref[0, k].astype(f32)
        p1 = pieces_ref[1, k].astype(f32)
        top = jnp.where(left, p0, pltpu.roll(p1, HD, 1))
        low = jnp.where(left, pltpu.roll(p0, HD, 1), p1)
        both = jnp.concatenate([top, low], axis=0)
        square = square + both * both
        gain = gain_ref[:, k * 2 * HD : (k + 1) * 2 * HD].astype(f32)
        scaled.append((both * gain).astype(jnp.bfloat16))
    u = jnp.concatenate(scaled, axis=1)
    r_in = lax.rsqrt(jnp.sum(square, axis=1, keepdims=True) / D + 1e-06)

    def times(weight, dims):
        return lax.dot_general(u, weight, dims, preferred_element_type=f32) * r_in

    across = (((1,), (1,)), ((), ()))
    down = (((1,), (0,)), ((), ()))
    x_rows = times(wx_ref[...], across).astype(jnp.bfloat16).astype(f32)
    b_rows = times(wb_ref[...], down).astype(jnp.bfloat16).astype(f32)
    c_rows = times(wc_ref[...], down).astype(jnp.bfloat16).astype(f32)
    z_rows = times(wz_ref[...], across).astype(jnp.bfloat16).astype(f32)
    dt_raw = times(wdt_ref[...], across)

    def wide(column):
        return jnp.broadcast_to(column, (seqs, 2 * HD))

    table = table_ref[...]
    parent = [wide(table[:, j : j + 1]) for j in range(PROP)]
    admitted = wide(table[:, PROP : PROP + 1])
    child = [[parent[j] == i for i in range(j)] for j in range(PROP)]

    def block(array, j):
        return array[j * seqs : (j + 1) * seqs]

    def conv(row_array, mem_ref, first):
        recent = []
        for back in range(CONV - 1):
            offset = CONV - 2 - back
            value = mem_ref[offset].astype(f32)
            for count in range(1, PREV + 1):
                value = jnp.where(admitted == count, mem_ref[offset + count].astype(f32), value)
            recent.append(value)
        history = []
        outs = []
        for j in range(PROP):
            inputs = [block(row_array, j)]
            for back in range(CONV - 1):
                value = recent[back]
                for i in range(j):
                    value = jnp.where(child[j][i], history[i][back], value)
                inputs.append(value)
            history.append(inputs)
            total = None
            for lag in range(CONV):
                tap = taps_ref[first + CONV - 1 - lag : first + CONV - lag, :]
                term = tap * inputs[lag]
                total = term if total is None else total + term
            outs.append(silu(total))
        return outs

    cc = conv(c_rows, mem_c_ref, 2 * CONV)
    for j in range(PROP):
        cc_all[:, j, :] = cc[j]
        cc_all[:, PROP + j, :] = cc[j]
    for s in range(seqs):
        read_all[s] = lax.dot_general(
            cc_all[s].astype(jnp.bfloat16), state_ref[s], across, preferred_element_type=f32
        )
    xc = conv(x_rows, mem_x_ref, 0)
    bc = conv(b_rows, mem_b_ref, CONV)

    offset = heads_ref[0:1, :]
    speed = heads_ref[1:2, :]
    bypass = heads_ref[2:3, :]
    fading = fading_ref[...]
    first_head = left[:seqs]
    level = []
    moved = []
    above = []
    for j in range(PROP):
        raw = block(dt_raw, j) + offset
        step = jnp.maximum(raw, 0.0) + jnp.log1p(jnp.exp(-jnp.abs(raw)))
        extra = jnp.where(
            first_head, wide(fading[:, 2 * j : 2 * j + 1]), wide(fading[:, 2 * j + 1 : 2 * j + 2])
        )
        own = speed * step + extra
        prior = jnp.zeros_like(own)
        for i in range(j):
            prior = jnp.where(child[j][i], level[i], prior)
        level.append(own + prior)
        moved.append(step * xc[j])
        line = []
        for i in range(j):
            reach = child[j][i]
            for p in range(i + 1, j):
                reach = reach | (child[j][p] & above[p][i])
            line.append(reach)
        above.append(line)
    for j in range(PROP):
        y = jnp.exp(level[j]) * read_all[:, j, :] + bypass * xc[j]
        for i in range(j + 1):
            score = jnp.sum(cc[j] * bc[i], axis=1, keepdims=True)
            if i == j:
                y = y + score * moved[i]
            else:
                fall = jnp.exp(jnp.minimum(level[j] - level[i], 0.0))
                y = y + jnp.where(above[j][i], fall * (score * moved[i]), 0.0)
        gated = (y * silu(block(z_rows, j))).astype(jnp.bfloat16)
        for copy in range(out_ref.shape[0]):
            out_ref[copy, j * seqs : (j + 1) * seqs, :] = gated


def last_kernel(tp_ref, own_ref, other_ref, weight_ref, out_ref, spread):
    f32 = jnp.float32
    kv_count, rows = own_ref.shape[0], own_ref.shape[1]
    seqs = rows // PROP
    group = tp_ref[0]
    total = jnp.zeros((rows, weight_ref.shape[1]), f32)
    square = jnp.zeros((rows, 2 * HD), f32)
    for k in range(kv_count):
        lhs = []
        rhs = []
        for ref, t in ((own_ref, group), (other_ref, 1 - group)):
            piece = ref[k]
            wide = piece.astype(f32)
            square = square + wide * wide
            lhs.append(piece)
            for h in range(2):
                start = pl.multiple_of(((2 * k + h) * G + t) * HD, HD)
                rhs.append(weight_ref[pl.ds(start, HD), :])
        total = total + jnp.dot(
            jnp.concatenate(lhs, axis=1), jnp.concatenate(rhs, axis=0), preferred_element_type=f32
        )
    r_out = lax.rsqrt(jnp.sum(square, axis=1, keepdims=True) / (HG * G * HD) + 1e-05)
    mixed = total * r_out
    for j in range(PROP):
        spread[:, j, :] = mixed[j * seqs : (j + 1) * seqs]
    out_ref[...] = spread[...].astype(jnp.bfloat16)


def pack(rows, copies):
    seqs = rows.shape[0]
    return pl.pallas_call(
        pack_kernel,
        out_shape=jax.ShapeDtypeStruct((copies, 2 * seqs, 2 * HD), jnp.bfloat16),
        in_specs=vmem(1),
        out_specs=vmem(1)[0],
        scratch_shapes=[pltpu.VMEM((PROP, seqs, HD), jnp.float32)],
        compiler_params=pltpu.CompilerParams(vmem_limit_bytes=8 << 20),
        interpret=INTERPRET,
        name="pack",
    )(rows)


def mixer(copies, pieces, *rest):
    half = pieces.shape[2]
    return pl.pallas_call(
        mixer_kernel,
        out_shape=jax.ShapeDtypeStruct((copies, 2 * half, 2 * HD), jnp.bfloat16),
        in_specs=vmem(1 + len(rest)),
        out_specs=vmem(1)[0],
        scratch_shapes=[
            pltpu.VMEM((half // 2, 2 * PROP, N), jnp.float32),
            pltpu.VMEM((half // 2, 2 * PROP, 2 * HD), jnp.float32),
        ],
        compiler_params=pltpu.CompilerParams(vmem_limit_bytes=20 << 20),
        cost_estimate=pl.CostEstimate(
            flops=2 * 2 * half * D * 5 * N, bytes_accessed=5 << 20, transcendentals=2 * half * 1000
        ),
        interpret=INTERPRET,
        name="mixer",
    )(pieces, *rest)


def last(group, own, other, weight):
    rows = own.shape[1]
    seqs = rows // PROP
    cols = weight.shape[1]
    return pl.pallas_call(
        last_kernel,
        out_shape=jax.ShapeDtypeStruct((seqs, PROP, cols), jnp.bfloat16),
        in_specs=[pl.BlockSpec(memory_space=pltpu.SMEM)] + vmem(3),
        out_specs=vmem(1)[0],
        scratch_shapes=[pltpu.VMEM((seqs, PROP, cols), jnp.float32)],
        compiler_params=pltpu.CompilerParams(vmem_limit_bytes=20 << 20),
        cost_estimate=pl.CostEstimate(
            flops=2 * rows * HG * G * HD * cols, bytes_accessed=2 << 20, transcendentals=rows
        ),
        interpret=INTERPRET,
        name="last",
    )(group, own, other, weight)


def prepared(
    kv_index,
    tp_index,
    leading_scaling_factor,
    lane_feed_matrix,
    final_valve_matrix,
    increment_matrix,
    entry_basis_matrix,
    readout_basis_matrix,
    lane_feed_kernel,
    entry_basis_kernel,
    readout_basis_kernel,
    increment_offset,
    shrink_speed_exponent,
    lane_bypass_factor,
    hidden_carried_memory,
    lane_filter_memory,
    entry_basis_memory,
    readout_basis_memory,
    predecessor_index,
    admitted_counts,
    surplus_fading,
):
    seqs = predecessor_index.shape[0]
    heads = increment_offset.shape[0]
    wx = jnp.transpose(lane_feed_matrix, (1, 2, 3, 0)).reshape(heads * HD, D)
    wz = jnp.transpose(final_valve_matrix, (1, 2, 3, 0)).reshape(heads * HD, D)
    dt_own = lax.dynamic_slice(
        jnp.transpose(increment_matrix, (1, 2, 0)), (kv_index * heads, tp_index, 0), (heads, 1, D)
    )
    wdt = jnp.broadcast_to(dt_own, (heads, HD, D)).reshape(heads * HD, D)
    wb = entry_basis_matrix.reshape(D, N)
    wc = readout_basis_matrix.reshape(D, N)
    taps = jnp.concatenate(
        [
            lane_feed_kernel.reshape(CONV, heads * HD),
            entry_basis_kernel.reshape(CONV, N),
            readout_basis_kernel.reshape(CONV, N),
        ],
        axis=0,
    )

    def per_lane(values):
        return jnp.broadcast_to(values, (heads, HD)).reshape(1, heads * HD)

    head_rows = jnp.concatenate(
        [
            per_lane(increment_offset),
            per_lane(-jnp.exp(shrink_speed_exponent)),
            per_lane(lane_bypass_factor),
        ],
        axis=0,
    )
    state = hidden_carried_memory.reshape(seqs, heads * HD, N).astype(jnp.bfloat16)
    mem_x = jnp.transpose(lane_filter_memory, (1, 0, 2, 3, 4)).reshape(WIN, seqs, heads * HD)
    mem_b = jnp.transpose(entry_basis_memory, (1, 0, 2, 3)).reshape(WIN, seqs, N)
    mem_c = jnp.transpose(readout_basis_memory, (1, 0, 2, 3)).reshape(WIN, seqs, N)
    table = jnp.concatenate([predecessor_index, admitted_counts[:, None]], axis=1)
    fading = surplus_fading.reshape(seqs, PROP * heads)
    return (
        leading_scaling_factor.reshape(1, D),
        wx,
        wz,
        wdt,
        wb,
        wc,
        taps,
        head_rows,
        state,
        mem_x,
        mem_b,
        mem_c,
        table,
        fading,
    )


def shards(candidate_vectors, leading_scaling_factor, lane_feed_matrix, final_valve_matrix,
           increment_matrix, entry_basis_matrix, readout_basis_matrix, lane_feed_kernel,
           entry_basis_kernel, readout_basis_kernel, increment_offset, shrink_speed_exponent,
           lane_bypass_factor, final_linear_matrix, *memories):
    kv_count = lax.axis_size("kv")
    copies = pack(candidate_vectors, kv_count)
    along = lax.all_to_all(copies, "kv", split_axis=0, concat_axis=0, tiled=True)
    pieces = lax.all_gather(along, "tp")
    rest = prepared(
        lax.axis_index("kv"), lax.axis_index("tp"), leading_scaling_factor, lane_feed_matrix,
        final_valve_matrix, increment_matrix, entry_basis_matrix, readout_basis_matrix,
        lane_feed_kernel, entry_basis_kernel, readout_basis_kernel, increment_offset,
        shrink_speed_exponent, lane_bypass_factor, *memories,
    )
    gated = mixer(1, pieces, *rest)
    along = lax.all_gather(gated[0], "kv")
    swapped = lax.ppermute(along, "tp", [(0, 1), (1, 0)])
    weight = final_linear_matrix.reshape(HG * G * HD, -1)
    return last(lax.axis_index("tp").reshape(1), along, swapped, weight)


def solution(mesh):
    placed = (
        P(("grp", "dp"), None, ("kv", "tp")),
        P(),
        P(None, "kv", "tp", None),
        P(None, "kv", "tp", None),
        P(),
        P(None, "tp", None),
        P(None, "tp", None),
        P(None, "kv", "tp", None),
        P(None, "tp", None),
        P(None, "tp", None),
        P("kv", "tp"),
        P("kv", "tp"),
        P("kv", "tp"),
        P(None, None, None, ("kv", "tp")),
        P(("grp", "dp"), "kv", "tp", None, None),
        P(("grp", "dp"), None, "kv", "tp", None),
        P(("grp", "dp"), None, "tp", None),
        P(("grp", "dp"), None, "tp", None),
        P(("grp", "dp"), None),
        P(("grp", "dp")),
        P(("grp", "dp"), None, "kv", "tp"),
    )
    return jax.shard_map(
        shards,
        mesh=mesh,
        in_specs=placed,
        out_specs=P(("grp", "dp"), None, ("kv", "tp")),
        check_vma=False,
    )
```

```python
import functools

import jax
import jax.numpy as jnp
from jax import lax
from jax.experimental import pallas as pl
from jax.experimental.pallas import tpu as pltpu
from jax.sharding import Mesh
from jax.sharding import PartitionSpec as P

D = 2048
HG = 32
G = 2
HD = 64
N = 128
CONV = 4
WIN = 7
PROP = 4
PREV = 4

KV = ("far", "near")

INTERPRET = False


def vmem(count):
    return [pl.BlockSpec(memory_space=pltpu.VMEM)] * count


def in_vmem(x):
    return x if INTERPRET else pltpu.with_memory_space_constraint(x, pltpu.VMEM)


def in_hbm(x):
    return x if INTERPRET else pltpu.with_memory_space_constraint(x, pltpu.HBM)


def pack_kernel(rows_ref, out_ref, wide):
    seqs = rows_ref.shape[0]
    for j in range(PROP):
        wide[j] = rows_ref[:, j, :].astype(jnp.float32)
    packed = jnp.concatenate(
        [
            jnp.concatenate([wide[0], wide[1]], axis=0),
            jnp.concatenate([wide[2], wide[3]], axis=0),
        ],
        axis=1,
    ).astype(jnp.bfloat16)
    for copy in range(out_ref.shape[0]):
        out_ref[copy] = packed


def places(seqs):
    at, row = {}, 0
    sizes = (("gain", D // N), ("taps", 16), ("heads", 8), ("fading", PROP * seqs), ("end", 0))
    for name, size in sizes:
        at[name] = row
        row += size
    return at


def prep_kernel(*refs):
    count = 13
    sources, held, sems = refs[:count], refs[count + 3 : -1], refs[-1]
    wide_out, narrow_out, recent_out = refs[count : count + 3]
    copies = [pltpu.make_async_copy(sources[k], held[k], sems.at[k]) for k in range(count)]
    for copy in copies:
        copy.start()
    (
        gain_ref,
        dt_ref,
        mem_x_ref,
        mem_b_ref,
        mem_c_ref,
        taps_x_ref,
        taps_b_ref,
        taps_c_ref,
        heads_ref,
        parents_ref,
        admitted_ref,
        fading_ref,
        state_ref,
    ) = held
    f32 = jnp.float32
    seqs = state_ref.shape[0]
    at = places(seqs)
    for copy in copies[:-1]:
        copy.wait()
    def put(name, index, value):
        start = at[name] + index * value.shape[0]
        wide_out[start : start + value.shape[0], :] = value

    for k in range(D // N):
        put("gain", k, gain_ref[:, k * N : (k + 1) * N].astype(f32))
        pair = [
            jnp.broadcast_to(dt_ref[h : h + 1, k * N : (k + 1) * N].astype(f32), (8, N))
            for h in range(2)
        ]
        row = (k % 8) * 16
        narrow_out[seqs + k // 8, row : row + 16, :] = jnp.concatenate(pair, axis=0).astype(
            jnp.bfloat16
        )
    for t in range(CONV):
        put("taps", t, jnp.concatenate([taps_x_ref[t, h] for h in range(2)], axis=1))
        put("taps", CONV + t, taps_b_ref[t])
        put("taps", 2 * CONV + t, taps_c_ref[t])
    one = lax.broadcasted_iota(jnp.int32, (1, 2 * HD), 1) < HD
    heads = heads_ref[...]
    for place in range(3):
        row = jnp.where(one, heads[place : place + 1, 0:1], heads[place : place + 1, 1:2])
        put("heads", place, -jnp.exp(row) if place == 1 else row)

    def turned(lines):
        total = sum(line.shape[0] for line in lines)
        if total < 8:
            lines = lines + [jnp.zeros((8 - total, seqs), f32)]
        lines = jnp.concatenate(lines, axis=0)
        lines = jnp.concatenate([lines, jnp.zeros((8, N - seqs), f32)], axis=1)
        return jnp.transpose(lines)[:seqs]

    def wide(column):
        return jnp.broadcast_to(column, (seqs, 2 * HD))

    table = turned([parents_ref[...].astype(f32), admitted_ref[...].astype(f32)])
    admitted = wide(table[:, PROP : PROP + 1])
    for j in range(PROP):
        start = 3 * (CONV - 1) + j
        recent_out[start * seqs : (start + 1) * seqs, :] = wide(table[:, j : j + 1]).astype(jnp.bfloat16)
    for which, mem_ref in enumerate((mem_x_ref, mem_b_ref, mem_c_ref)):
        for back in range(CONV - 1):
            offset = CONV - 2 - back
            value = mem_ref[offset].astype(f32)
            for step in range(1, PREV + 1):
                value = jnp.where(admitted == step, mem_ref[offset + step].astype(f32), value)
            start = which * (CONV - 1) + back
            recent_out[start * seqs : (start + 1) * seqs, :] = value.astype(jnp.bfloat16)
    fading = turned([fading_ref[j, h] for j in range(PROP) for h in range(2)])
    first_head = lax.broadcasted_iota(jnp.int32, (seqs, 2 * HD), 1) < HD
    for j in range(PROP):
        pair = [wide(fading[:, 2 * j + h : 2 * j + h + 1]) for h in range(2)]
        put("fading", j, jnp.where(first_head, *pair))
    copies[-1].wait()
    narrow_out[:seqs] = state_ref[...].astype(jnp.bfloat16)


def mixer_kernel(
    pieces_ref,
    wx_ref,
    wz_ref,
    wb_ref,
    wc_ref,
    wide_ref,
    narrow_ref,
    recent_ref,
    out_ref,
    cc_all,
    read_all,
    wz_held,
    wz_sem,
):
    half = pieces_ref.shape[2]
    seqs = half // 2
    rows = 2 * half
    kv_count = pieces_ref.shape[1]
    f32 = jnp.float32
    wz_copy = pltpu.make_async_copy(wz_ref, wz_held, wz_sem)
    wz_copy.start()
    left = lax.broadcasted_iota(jnp.int32, (half, 2 * HD), 1) < HD
    at = places(seqs)

    def table(name, index, size):
        return wide_ref[at[name] + index * size : at[name] + (index + 1) * size, :]

    scaled = []
    square = jnp.zeros((rows, 2 * HD), f32)
    for k in range(kv_count):
        p0 = pieces_ref[0, k].astype(f32)
        p1 = pieces_ref[1, k].astype(f32)
        top = jnp.where(left, p0, pltpu.roll(p1, HD, 1))
        low = jnp.where(left, pltpu.roll(p0, HD, 1), p1)
        both = jnp.concatenate([top, low], axis=0)
        square = square + both * both
        gain = table("gain", k, 1)
        scaled.append((both * gain).astype(jnp.bfloat16))
    u = jnp.concatenate(scaled, axis=1)
    r_in = lax.rsqrt(jnp.sum(square, axis=1, keepdims=True) / D + 1e-06)

    def times(weight, dims):
        return lax.dot_general(u, weight, dims, preferred_element_type=f32) * r_in

    across = (((1,), (1,)), ((), ()))
    down = (((1,), (0,)), ((), ()))
    c_rows = times(wc_ref[...], down).astype(jnp.bfloat16).astype(f32)
    b_rows = times(wb_ref[...], down).astype(jnp.bfloat16).astype(f32)
    x_rows = times(wx_ref[...], across).astype(jnp.bfloat16).astype(f32)
    chunks = [narrow_ref[seqs + k // 8, (k % 8) * 16 : (k % 8) * 16 + 16, :] for k in range(D // N)]
    dt_cols = times(jnp.concatenate(chunks, axis=1), across)
    dt_raw = jnp.where(
        lax.broadcasted_iota(jnp.int32, (rows, 2 * HD), 1) < HD,
        *(jnp.broadcast_to(dt_cols[:, c : c + 1], (rows, 2 * HD)) for c in (0, 8)),
    )

    def recent(index):
        return recent_ref[index * seqs : (index + 1) * seqs, :].astype(f32)

    parent = [recent(3 * (CONV - 1) + j) for j in range(PROP)]
    child = [[parent[j] == i for i in range(j)] for j in range(PROP)]

    def block(array, j):
        return array[j * seqs : (j + 1) * seqs]

    def conv(row_array, which):
        history = []
        outs = []
        roots = [recent(which * (CONV - 1) + back) for back in range(CONV - 1)]
        for j in range(PROP):
            inputs = [block(row_array, j)]
            for back in range(CONV - 1):
                value = roots[back]
                for i in range(j):
                    value = jnp.where(child[j][i], history[i][back], value)
                inputs.append(value)
            history.append(inputs)
            total = None
            for lag in range(CONV):
                term = table("taps", which * CONV + CONV - 1 - lag, 1) * inputs[lag]
                total = term if total is None else total + term
            outs.append(jax.nn.silu(total))
        return outs

    cc = conv(c_rows, 2)
    for j in range(PROP):
        cc_all[:, j, :] = cc[j]
        cc_all[:, PROP + j, :] = cc[j]
    for s in range(seqs):
        read_all[s] = lax.dot_general(
            cc_all[s].astype(jnp.bfloat16), narrow_ref[s], across, preferred_element_type=f32
        )
    xc = conv(x_rows, 0)
    bc = conv(b_rows, 1)

    offset, speed, bypass = (table("heads", place, 1) for place in range(3))
    level = []
    moved = []
    above = []
    for j in range(PROP):
        raw = block(dt_raw, j) + offset
        step = jnp.maximum(raw, 0.0) + jnp.log1p(jnp.exp(-jnp.abs(raw)))
        own = speed * step + table("fading", j, seqs)
        prior = jnp.zeros_like(own)
        for i in range(j):
            prior = jnp.where(child[j][i], level[i], prior)
        level.append(own + prior)
        moved.append(step * xc[j])
        line = []
        for i in range(j):
            reach = child[j][i]
            for p in range(i + 1, j):
                reach = reach | (child[j][p] & above[p][i])
            line.append(reach)
        above.append(line)
    wz_copy.wait()
    z_rows = times(wz_held[...], across).astype(jnp.bfloat16).astype(f32)
    for j in range(PROP):
        y = jnp.exp(level[j]) * read_all[:, j, :] + bypass * xc[j]
        for i in range(j + 1):
            score = jnp.sum(cc[j] * bc[i], axis=1, keepdims=True)
            if i == j:
                y = y + score * moved[i]
            else:
                fall = jnp.exp(jnp.minimum(level[j] - level[i], 0.0))
                y = y + jnp.where(above[j][i], fall * (score * moved[i]), 0.0)
        gated = (y * jax.nn.silu(block(z_rows, j))).astype(jnp.bfloat16)
        out_ref[j * seqs : (j + 1) * seqs, :] = gated


def last_kernel(tp_ref, own_ref, other_ref, weight_ref, out_ref, spread):
    f32 = jnp.float32
    near, far, rows = own_ref.shape[:3]
    seqs = rows // PROP
    group = tp_ref[0]
    total = jnp.zeros((rows, weight_ref.shape[1]), f32)
    square = jnp.zeros((rows, 2 * HD), f32)
    for k in range(near * far):
        lhs = []
        rhs = []
        for ref, t in ((own_ref, group), (other_ref, 1 - group)):
            piece = ref[k % near, k // near]
            wide = piece.astype(f32)
            square = square + wide * wide
            lhs.append(piece)
            for h in range(2):
                start = pl.multiple_of(((2 * k + h) * G + t) * HD, HD)
                rhs.append(weight_ref[pl.ds(start, HD), :])
        total = total + jnp.dot(
            jnp.concatenate(lhs, axis=1), jnp.concatenate(rhs, axis=0), preferred_element_type=f32
        )
    r_out = lax.rsqrt(jnp.sum(square, axis=1, keepdims=True) / (HG * G * HD) + 1e-05)
    mixed = total * r_out
    for j in range(PROP):
        spread[:, j, :] = mixed[j * seqs : (j + 1) * seqs]
    out_ref[...] = spread[...].astype(jnp.bfloat16)


def pack(rows, copies):
    seqs = rows.shape[0]
    return pl.pallas_call(
        pack_kernel,
        out_shape=jax.ShapeDtypeStruct((copies, 2 * seqs, 2 * HD), jnp.bfloat16),
        in_specs=vmem(1),
        out_specs=vmem(1)[0],
        scratch_shapes=[pltpu.VMEM((PROP, seqs, HD), jnp.float32)],
        compiler_params=pltpu.CompilerParams(vmem_limit_bytes=8 << 20),
        interpret=INTERPRET,
        name="pack",
    )(rows)


def prep(*inputs):
    state = inputs[-1]
    seqs = state.shape[0]
    return pl.pallas_call(
        prep_kernel,
        out_shape=[
            pltpu.VMEM((places(seqs)["end"], N), jnp.float32),
            pltpu.VMEM((seqs + D // N // 8, N, N), jnp.bfloat16),
            pltpu.VMEM(((3 * (CONV - 1) + PROP) * seqs, N), jnp.bfloat16),
        ],
        in_specs=[pl.BlockSpec(memory_space=pltpu.HBM)] * len(inputs),
        out_specs=vmem(3),
        scratch_shapes=[pltpu.VMEM(x.shape, x.dtype) for x in inputs]
        + [pltpu.SemaphoreType.DMA((len(inputs),))],
        compiler_params=pltpu.CompilerParams(vmem_limit_bytes=16 << 20),
        cost_estimate=pl.CostEstimate(flops=1 << 24, bytes_accessed=4 << 20, transcendentals=0),
        interpret=INTERPRET,
        name="prep",
    )(*(in_hbm(x) for x in inputs))


def mixer(pieces, *rest):
    half = pieces.shape[2]
    return pl.pallas_call(
        mixer_kernel,
        out_shape=jax.ShapeDtypeStruct((2 * half, 2 * HD), jnp.bfloat16),
        in_specs=vmem(2) + [pl.BlockSpec(memory_space=pltpu.HBM)] + vmem(len(rest) - 2),
        out_specs=vmem(1)[0],
        scratch_shapes=[
            pltpu.VMEM((half // 2, 2 * PROP, N), jnp.float32),
            pltpu.VMEM((half // 2, 2 * PROP, 2 * HD), jnp.float32),
            pltpu.VMEM((2 * HD, D), jnp.bfloat16),
            pltpu.SemaphoreType.DMA,
        ],
        compiler_params=pltpu.CompilerParams(vmem_limit_bytes=20 << 20),
        cost_estimate=pl.CostEstimate(
            flops=2 * 2 * half * D * 5 * N, bytes_accessed=5 << 20, transcendentals=2 * half * 1000
        ),
        interpret=INTERPRET,
        name="mixer",
    )(pieces, *rest)


def last(group, own, other, weight):
    rows = own.shape[2]
    seqs = rows // PROP
    cols = weight.shape[1]
    return pl.pallas_call(
        last_kernel,
        out_shape=jax.ShapeDtypeStruct((seqs, PROP, cols), jnp.bfloat16),
        in_specs=[pl.BlockSpec(memory_space=pltpu.SMEM)] + vmem(3),
        out_specs=vmem(1)[0],
        scratch_shapes=[pltpu.VMEM((seqs, PROP, cols), jnp.float32)],
        compiler_params=pltpu.CompilerParams(vmem_limit_bytes=20 << 20),
        cost_estimate=pl.CostEstimate(
            flops=2 * rows * HG * G * HD * cols, bytes_accessed=2 << 20, transcendentals=rows
        ),
        interpret=INTERPRET,
        name="last",
    )(group, own, other, weight)


def prepared(
    kv_index,
    tp_index,
    leading_scaling_factor,
    lane_feed_matrix,
    final_valve_matrix,
    increment_matrix,
    entry_basis_matrix,
    readout_basis_matrix,
    lane_feed_kernel,
    entry_basis_kernel,
    readout_basis_kernel,
    increment_offset,
    shrink_speed_exponent,
    lane_bypass_factor,
    hidden_carried_memory,
    lane_filter_memory,
    entry_basis_memory,
    readout_basis_memory,
    predecessor_index,
    admitted_counts,
    surplus_fading,
):
    seqs = predecessor_index.shape[0]
    heads = increment_offset.shape[0]
    wx = jnp.transpose(lane_feed_matrix, (1, 2, 3, 0)).reshape(heads * HD, D)
    wz = jnp.transpose(final_valve_matrix, (1, 2, 3, 0)).reshape(heads * HD, D)
    dt_own = lax.dynamic_slice(
        jnp.transpose(increment_matrix, (1, 2, 0)), (kv_index * heads, tp_index, 0), (heads, 1, D)
    )
    wb = entry_basis_matrix.reshape(D, N)
    wc = readout_basis_matrix.reshape(D, N)
    head_rows = jnp.stack(
        [x.reshape(heads) for x in (increment_offset, shrink_speed_exponent, lane_bypass_factor)]
    )
    ready = prep(
        leading_scaling_factor.reshape(1, D),
        dt_own.reshape(heads, D),
        jnp.transpose(lane_filter_memory, (1, 0, 2, 3, 4)).reshape(WIN, seqs, heads * HD),
        jnp.transpose(entry_basis_memory, (1, 0, 2, 3)).reshape(WIN, seqs, N),
        jnp.transpose(readout_basis_memory, (1, 0, 2, 3)).reshape(WIN, seqs, N),
        lane_feed_kernel,
        entry_basis_kernel,
        readout_basis_kernel,
        head_rows,
        jnp.transpose(predecessor_index),
        admitted_counts.reshape(1, seqs),
        jnp.transpose(surplus_fading, (1, 2, 3, 0)),
        hidden_carried_memory.reshape(seqs, heads * HD, N),
    )
    return (wx, in_hbm(wz), wb, wc, *(in_vmem(x) for x in ready))


def shards(candidate_vectors, leading_scaling_factor, lane_feed_matrix, final_valve_matrix,
           increment_matrix, entry_basis_matrix, readout_basis_matrix, lane_feed_kernel,
           entry_basis_kernel, readout_basis_kernel, increment_offset, shrink_speed_exponent,
           lane_bypass_factor, final_linear_matrix, *memories):
    copies = pack(candidate_vectors, lax.axis_size(KV))
    along = lax.all_to_all(copies, KV, split_axis=0, concat_axis=0, tiled=True)
    pieces = lax.all_gather(along, "tp")
    rest = prepared(
        lax.axis_index(KV), lax.axis_index("tp"), leading_scaling_factor, lane_feed_matrix,
        final_valve_matrix, increment_matrix, entry_basis_matrix, readout_basis_matrix,
        lane_feed_kernel, entry_basis_kernel, readout_basis_kernel, increment_offset,
        shrink_speed_exponent, lane_bypass_factor, *memories,
    )
    gated = mixer(pieces, *rest)
    far = lax.all_gather(gated, "far")
    along = lax.all_gather(far, "near")
    swapped = lax.ppermute(along, "tp", [(0, 1), (1, 0)])
    weight = final_linear_matrix.reshape(HG * G * HD, -1)
    return last(lax.axis_index("tp").reshape(1), along, swapped, weight)


def solution(mesh):
    grp, dp, kv, tp = (mesh.shape[axis] for axis in ("grp", "dp", "kv", "tp"))
    near = 4 if kv % 4 == 0 else 1
    split = Mesh(mesh.devices.reshape(grp, dp, kv // near, near, tp), ("grp", "dp", *KV, "tp"))
    placed = (
        P(("grp", "dp"), None, (*KV, "tp")),
        P(),
        P(None, KV, "tp", None),
        P(None, KV, "tp", None),
        P(),
        P(None, "tp", None),
        P(None, "tp", None),
        P(None, KV, "tp", None),
        P(None, "tp", None),
        P(None, "tp", None),
        P(KV, "tp"),
        P(KV, "tp"),
        P(KV, "tp"),
        P(None, None, None, (*KV, "tp")),
        P(("grp", "dp"), KV, "tp", None, None),
        P(("grp", "dp"), None, KV, "tp", None),
        P(("grp", "dp"), None, "tp", None),
        P(("grp", "dp"), None, "tp", None),
        P(("grp", "dp"), None),
        P(("grp", "dp")),
        P(("grp", "dp"), None, KV, "tp"),
    )
    return jax.shard_map(
        shards,
        mesh=split,
        in_specs=placed,
        out_specs=P(("grp", "dp"), None, (*KV, "tp")),
        check_vma=False,
    )
```

```python
import functools

import jax
import jax.numpy as jnp
from jax import lax
from jax.experimental import pallas as pl
from jax.experimental.pallas import tpu as pltpu
from jax.sharding import PartitionSpec as P

D = 2048
HG = 32
G = 2
HD = 64
N = 128
CONV = 4
WIN = 7
PROP = 4
PREV = 4

KV = "kv"

INTERPRET = False


def vmem(count):
    return [pl.BlockSpec(memory_space=pltpu.VMEM)] * count


def in_vmem(x):
    return x if INTERPRET else pltpu.with_memory_space_constraint(x, pltpu.VMEM)


def in_hbm(x):
    return x if INTERPRET else pltpu.with_memory_space_constraint(x, pltpu.HBM)


def pack_kernel(rows_ref, out_ref, wide):
    seqs = rows_ref.shape[0]
    for j in range(PROP):
        wide[j] = rows_ref[:, j, :].astype(jnp.float32)
    packed = jnp.concatenate(
        [
            jnp.concatenate([wide[0], wide[1]], axis=0),
            jnp.concatenate([wide[2], wide[3]], axis=0),
        ],
        axis=1,
    ).astype(jnp.bfloat16)
    for copy in range(out_ref.shape[0]):
        out_ref[copy] = packed


def places(seqs):
    at, row = {}, 0
    sizes = (("taps", 16), ("heads", 8), ("fading", PROP * seqs), ("end", 0))
    for name, size in sizes:
        at[name] = row
        row += size
    return at


def prep_kernel(*refs):
    count = 13
    sources, held, sems = refs[:count], refs[count + 3 : -1], refs[-1]
    wide_out, narrow_out, recent_out = refs[count : count + 3]
    copies = [pltpu.make_async_copy(sources[k], held[k], sems.at[k]) for k in range(count)]
    for copy in copies:
        copy.start()
    (
        gain_ref,
        dt_ref,
        mem_x_ref,
        mem_b_ref,
        mem_c_ref,
        taps_x_ref,
        taps_b_ref,
        taps_c_ref,
        heads_ref,
        parents_ref,
        admitted_ref,
        fading_ref,
        state_ref,
    ) = held
    f32 = jnp.float32
    seqs = state_ref.shape[0]
    at = places(seqs)
    for copy in copies[:-1]:
        copy.wait()
    def put(name, index, value):
        start = at[name] + index * value.shape[0]
        wide_out[start : start + value.shape[0], :] = value

    for k in range(D // N):
        pair = [
            jnp.broadcast_to(dt_ref[h : h + 1, k * N : (k + 1) * N].astype(f32), (8, N))
            for h in range(2)
        ]
        row = (k % 8) * 16
        narrow_out[seqs + k // 8, row : row + 16, :] = jnp.concatenate(pair, axis=0).astype(
            jnp.bfloat16
        )
    gains = [gain_ref[:, k * N : (k + 1) * N].astype(f32) for k in range(D // N)]
    narrow_out[seqs + D // N // 8, : D // N, :] = jnp.concatenate(gains, axis=0).astype(jnp.bfloat16)
    for t in range(CONV):
        put("taps", t, jnp.concatenate([taps_x_ref[t, h] for h in range(2)], axis=1))
        put("taps", CONV + t, taps_b_ref[t])
        put("taps", 2 * CONV + t, taps_c_ref[t])
    one = lax.broadcasted_iota(jnp.int32, (1, 2 * HD), 1) < HD
    heads = heads_ref[...]
    for place in range(3):
        row = jnp.where(one, heads[place : place + 1, 0:1], heads[place : place + 1, 1:2])
        put("heads", place, -jnp.exp(row) if place == 1 else row)

    def turned(lines):
        total = sum(line.shape[0] for line in lines)
        if total < 8:
            lines = lines + [jnp.zeros((8 - total, seqs), f32)]
        lines = jnp.concatenate(lines, axis=0)
        lines = jnp.concatenate([lines, jnp.zeros((8, N - seqs), f32)], axis=1)
        return jnp.transpose(lines)[:seqs]

    def wide(column):
        return jnp.broadcast_to(column, (seqs, 2 * HD))

    table = turned([parents_ref[...].astype(f32), admitted_ref[...].astype(f32)])
    admitted = wide(table[:, PROP : PROP + 1])
    for j in range(PROP):
        start = 3 * (CONV - 1) + j
        recent_out[start * seqs : (start + 1) * seqs, :] = wide(table[:, j : j + 1]).astype(jnp.bfloat16)
    for which, mem_ref in enumerate((mem_x_ref, mem_b_ref, mem_c_ref)):
        for back in range(CONV - 1):
            offset = CONV - 2 - back
            value = mem_ref[offset].astype(f32)
            for step in range(1, PREV + 1):
                value = jnp.where(admitted == step, mem_ref[offset + step].astype(f32), value)
            start = which * (CONV - 1) + back
            recent_out[start * seqs : (start + 1) * seqs, :] = value.astype(jnp.bfloat16)
    fading = turned([fading_ref[j, h] for j in range(PROP) for h in range(2)])
    first_head = lax.broadcasted_iota(jnp.int32, (seqs, 2 * HD), 1) < HD
    for j in range(PROP):
        pair = [wide(fading[:, 2 * j + h : 2 * j + h + 1]) for h in range(2)]
        put("fading", j, jnp.where(first_head, *pair))
    copies[-1].wait()
    narrow_out[:seqs] = state_ref[...].astype(jnp.bfloat16)


def mixer_kernel(
    pieces_ref,
    wx_ref,
    wz_ref,
    wb_ref,
    wc_ref,
    narrow_ref,
    wide_far,
    recent_far,
    out_ref,
    cc_all,
    read_all,
    wide_ref,
    recent_ref,
    sems,
):
    half = pieces_ref.shape[2]
    seqs = half // 2
    rows = 2 * half
    kv_count = pieces_ref.shape[1]
    f32 = jnp.float32
    copies = [
        pltpu.make_async_copy(wide_far, wide_ref, sems.at[0]),
        pltpu.make_async_copy(recent_far, recent_ref, sems.at[1]),
    ]
    for copy in copies:
        copy.start()
    left = lax.broadcasted_iota(jnp.int32, (half, 2 * HD), 1) < HD
    at = places(seqs)

    def table(name, index, size):
        return wide_ref[at[name] + index * size : at[name] + (index + 1) * size, :]

    gains = narrow_ref[seqs + D // N // 8, : D // N, :].astype(f32)
    scaled = []
    square = jnp.zeros((rows, 2 * HD), f32)
    for k in range(kv_count):
        p0 = pieces_ref[0, k].astype(f32)
        p1 = pieces_ref[1, k].astype(f32)
        top = jnp.where(left, p0, pltpu.roll(p1, HD, 1))
        low = jnp.where(left, pltpu.roll(p0, HD, 1), p1)
        both = jnp.concatenate([top, low], axis=0)
        square = square + both * both
        gain = gains[k : k + 1, :]
        scaled.append((both * gain).astype(jnp.bfloat16))
    u = jnp.concatenate(scaled, axis=1)
    r_in = lax.rsqrt(jnp.sum(square, axis=1, keepdims=True) / D + 1e-06)

    def times(weight, dims):
        return lax.dot_general(u, weight, dims, preferred_element_type=f32) * r_in

    across = (((1,), (1,)), ((), ()))
    down = (((1,), (0,)), ((), ()))
    c_rows = times(wc_ref[...], down).astype(jnp.bfloat16).astype(f32)
    b_rows = times(wb_ref[...], down).astype(jnp.bfloat16).astype(f32)
    x_rows = times(wx_ref[...], across).astype(jnp.bfloat16).astype(f32)
    z_rows = times(wz_ref[...], across).astype(jnp.bfloat16).astype(f32)
    chunks = [narrow_ref[seqs + k // 8, (k % 8) * 16 : (k % 8) * 16 + 16, :] for k in range(D // N)]
    dt_cols = times(jnp.concatenate(chunks, axis=1), across)
    dt_raw = jnp.where(
        lax.broadcasted_iota(jnp.int32, (rows, 2 * HD), 1) < HD,
        *(jnp.broadcast_to(dt_cols[:, c : c + 1], (rows, 2 * HD)) for c in (0, 8)),
    )

    for copy in copies:
        copy.wait()

    def recent(index):
        return recent_ref[index * seqs : (index + 1) * seqs, :].astype(f32)

    parent = [recent(3 * (CONV - 1) + j) for j in range(PROP)]
    child = [[parent[j] == i for i in range(j)] for j in range(PROP)]

    def block(array, j):
        return array[j * seqs : (j + 1) * seqs]

    def conv(row_array, which):
        history = []
        outs = []
        roots = [recent(which * (CONV - 1) + back) for back in range(CONV - 1)]
        for j in range(PROP):
            inputs = [block(row_array, j)]
            for back in range(CONV - 1):
                value = roots[back]
                for i in range(j):
                    value = jnp.where(child[j][i], history[i][back], value)
                inputs.append(value)
            history.append(inputs)
            total = None
            for lag in range(CONV):
                term = table("taps", which * CONV + CONV - 1 - lag, 1) * inputs[lag]
                total = term if total is None else total + term
            outs.append(jax.nn.silu(total))
        return outs

    cc = conv(c_rows, 2)
    for j in range(PROP):
        cc_all[:, j, :] = cc[j]
        cc_all[:, PROP + j, :] = cc[j]
    for s in range(seqs):
        read_all[s] = lax.dot_general(
            cc_all[s].astype(jnp.bfloat16), narrow_ref[s], across, preferred_element_type=f32
        )
    xc = conv(x_rows, 0)
    bc = conv(b_rows, 1)

    offset, speed, bypass = (table("heads", place, 1) for place in range(3))
    level = []
    moved = []
    above = []
    for j in range(PROP):
        raw = block(dt_raw, j) + offset
        step = jnp.maximum(raw, 0.0) + jnp.log1p(jnp.exp(-jnp.abs(raw)))
        own = speed * step + table("fading", j, seqs)
        prior = jnp.zeros_like(own)
        for i in range(j):
            prior = jnp.where(child[j][i], level[i], prior)
        level.append(own + prior)
        moved.append(step * xc[j])
        line = []
        for i in range(j):
            reach = child[j][i]
            for p in range(i + 1, j):
                reach = reach | (child[j][p] & above[p][i])
            line.append(reach)
        above.append(line)
    for j in range(PROP):
        y = jnp.exp(level[j]) * read_all[:, j, :] + bypass * xc[j]
        for i in range(j + 1):
            score = jnp.sum(cc[j] * bc[i], axis=1, keepdims=True)
            if i == j:
                y = y + score * moved[i]
            else:
                fall = jnp.exp(jnp.minimum(level[j] - level[i], 0.0))
                y = y + jnp.where(above[j][i], fall * (score * moved[i]), 0.0)
        gated = (y * jax.nn.silu(block(z_rows, j))).astype(jnp.bfloat16)
        out_ref[j * seqs : (j + 1) * seqs, :] = gated


def last_kernel(tp_ref, own_ref, other_ref, weight_ref, out_ref, spread):
    f32 = jnp.float32
    kv_count, rows = own_ref.shape[:2]
    seqs = rows // PROP
    group = tp_ref[0]
    total = jnp.zeros((rows, weight_ref.shape[1]), f32)
    square = jnp.zeros((rows, 2 * HD), f32)
    for k in range(kv_count):
        lhs = []
        rhs = []
        for ref, t in ((own_ref, group), (other_ref, 1 - group)):
            piece = ref[k]
            wide = piece.astype(f32)
            square = square + wide * wide
            lhs.append(piece)
            for h in range(2):
                start = pl.multiple_of(((2 * k + h) * G + t) * HD, HD)
                rhs.append(weight_ref[pl.ds(start, HD), :])
        total = total + jnp.dot(
            jnp.concatenate(lhs, axis=1), jnp.concatenate(rhs, axis=0), preferred_element_type=f32
        )
    r_out = lax.rsqrt(jnp.sum(square, axis=1, keepdims=True) / (HG * G * HD) + 1e-05)
    mixed = total * r_out
    for j in range(PROP):
        spread[:, j, :] = mixed[j * seqs : (j + 1) * seqs]
    out_ref[...] = spread[...].astype(jnp.bfloat16)


def pack(rows, copies):
    seqs = rows.shape[0]
    return pl.pallas_call(
        pack_kernel,
        out_shape=jax.ShapeDtypeStruct((copies, 2 * seqs, 2 * HD), jnp.bfloat16),
        in_specs=vmem(1),
        out_specs=vmem(1)[0],
        scratch_shapes=[pltpu.VMEM((PROP, seqs, HD), jnp.float32)],
        compiler_params=pltpu.CompilerParams(vmem_limit_bytes=8 << 20),
        interpret=INTERPRET,
        name="pack",
    )(rows)


def prep(*inputs):
    state = inputs[-1]
    seqs = state.shape[0]
    return pl.pallas_call(
        prep_kernel,
        out_shape=[
            jax.ShapeDtypeStruct((places(seqs)["end"], N), jnp.float32),
            pltpu.VMEM((seqs + D // N // 8 + 1, N, N), jnp.bfloat16),
            jax.ShapeDtypeStruct(((3 * (CONV - 1) + PROP) * seqs, N), jnp.bfloat16),
        ],
        in_specs=[pl.BlockSpec(memory_space=pltpu.HBM)] * len(inputs),
        out_specs=vmem(3),
        scratch_shapes=[pltpu.VMEM(x.shape, x.dtype) for x in inputs]
        + [pltpu.SemaphoreType.DMA((len(inputs),))],
        compiler_params=pltpu.CompilerParams(vmem_limit_bytes=16 << 20),
        cost_estimate=pl.CostEstimate(flops=1 << 24, bytes_accessed=4 << 20, transcendentals=0),
        interpret=INTERPRET,
        name="prep",
    )(*(in_hbm(x) for x in inputs))


def mixer(pieces, *rest):
    half = pieces.shape[2]
    return pl.pallas_call(
        mixer_kernel,
        out_shape=jax.ShapeDtypeStruct((2 * half, 2 * HD), jnp.bfloat16),
        in_specs=vmem(6) + [pl.BlockSpec(memory_space=pltpu.HBM)] * 2,
        out_specs=vmem(1)[0],
        scratch_shapes=[
            pltpu.VMEM((half // 2, 2 * PROP, N), jnp.float32),
            pltpu.VMEM((half // 2, 2 * PROP, 2 * HD), jnp.float32),
            *(pltpu.VMEM(x.shape, x.dtype) for x in rest[-2:]),
            pltpu.SemaphoreType.DMA((2,)),
        ],
        compiler_params=pltpu.CompilerParams(vmem_limit_bytes=20 << 20),
        cost_estimate=pl.CostEstimate(
            flops=2 * 2 * half * D * 5 * N, bytes_accessed=5 << 20, transcendentals=2 * half * 1000
        ),
        interpret=INTERPRET,
        name="mixer",
    )(pieces, *rest)


def last(group, own, other, weight):
    rows = own.shape[1]
    seqs = rows // PROP
    cols = weight.shape[1]
    return pl.pallas_call(
        last_kernel,
        out_shape=jax.ShapeDtypeStruct((seqs, PROP, cols), jnp.bfloat16),
        in_specs=[pl.BlockSpec(memory_space=pltpu.SMEM)] + vmem(3),
        out_specs=vmem(1)[0],
        scratch_shapes=[pltpu.VMEM((seqs, PROP, cols), jnp.float32)],
        compiler_params=pltpu.CompilerParams(vmem_limit_bytes=20 << 20),
        cost_estimate=pl.CostEstimate(
            flops=2 * rows * HG * G * HD * cols, bytes_accessed=2 << 20, transcendentals=rows
        ),
        interpret=INTERPRET,
        name="last",
    )(group, own, other, weight)


def prepared(
    kv_index,
    tp_index,
    leading_scaling_factor,
    lane_feed_matrix,
    final_valve_matrix,
    increment_matrix,
    entry_basis_matrix,
    readout_basis_matrix,
    lane_feed_kernel,
    entry_basis_kernel,
    readout_basis_kernel,
    increment_offset,
    shrink_speed_exponent,
    lane_bypass_factor,
    hidden_carried_memory,
    lane_filter_memory,
    entry_basis_memory,
    readout_basis_memory,
    predecessor_index,
    admitted_counts,
    surplus_fading,
):
    seqs = predecessor_index.shape[0]
    heads = increment_offset.shape[0]
    wx = jnp.transpose(lane_feed_matrix, (1, 2, 3, 0)).reshape(heads * HD, D)
    wz = jnp.transpose(final_valve_matrix, (1, 2, 3, 0)).reshape(heads * HD, D)
    dt_own = lax.dynamic_slice(
        jnp.transpose(increment_matrix, (1, 2, 0)), (kv_index * heads, tp_index, 0), (heads, 1, D)
    )
    wb = entry_basis_matrix.reshape(D, N)
    wc = readout_basis_matrix.reshape(D, N)
    head_rows = jnp.stack(
        [x.reshape(heads) for x in (increment_offset, shrink_speed_exponent, lane_bypass_factor)]
    )
    wide, narrow, recent = prep(
        leading_scaling_factor.reshape(1, D),
        dt_own.reshape(heads, D),
        jnp.transpose(lane_filter_memory, (1, 0, 2, 3, 4)).reshape(WIN, seqs, heads * HD),
        jnp.transpose(entry_basis_memory, (1, 0, 2, 3)).reshape(WIN, seqs, N),
        jnp.transpose(readout_basis_memory, (1, 0, 2, 3)).reshape(WIN, seqs, N),
        lane_feed_kernel,
        entry_basis_kernel,
        readout_basis_kernel,
        head_rows,
        jnp.transpose(predecessor_index),
        admitted_counts.reshape(1, seqs),
        jnp.transpose(surplus_fading, (1, 2, 3, 0)),
        hidden_carried_memory.reshape(seqs, heads * HD, N),
    )
    return (wx, wz, wb, wc, in_vmem(narrow), in_hbm(wide), in_hbm(recent))


def shards(candidate_vectors, leading_scaling_factor, lane_feed_matrix, final_valve_matrix,
           increment_matrix, entry_basis_matrix, readout_basis_matrix, lane_feed_kernel,
           entry_basis_kernel, readout_basis_kernel, increment_offset, shrink_speed_exponent,
           lane_bypass_factor, final_linear_matrix, *memories):
    copies = pack(candidate_vectors, lax.axis_size(KV))
    along = lax.all_to_all(copies, KV, split_axis=0, concat_axis=0, tiled=True)
    pieces = lax.all_gather(along, "tp")
    rest = prepared(
        lax.axis_index(KV), lax.axis_index("tp"), leading_scaling_factor, lane_feed_matrix,
        final_valve_matrix, increment_matrix, entry_basis_matrix, readout_basis_matrix,
        lane_feed_kernel, entry_basis_kernel, readout_basis_kernel, increment_offset,
        shrink_speed_exponent, lane_bypass_factor, *memories,
    )
    gated = mixer(pieces, *rest)
    along = lax.all_gather(gated, KV)
    swapped = lax.ppermute(along, "tp", [(0, 1), (1, 0)])
    weight = final_linear_matrix.reshape(HG * G * HD, -1)
    return last(lax.axis_index("tp").reshape(1), along, swapped, weight)


def solution(mesh):
    placed = (
        P(("grp", "dp"), None, ("kv", "tp")),
        P(),
        P(None, KV, "tp", None),
        P(None, KV, "tp", None),
        P(),
        P(None, "tp", None),
        P(None, "tp", None),
        P(None, KV, "tp", None),
        P(None, "tp", None),
        P(None, "tp", None),
        P(KV, "tp"),
        P(KV, "tp"),
        P(KV, "tp"),
        P(None, None, None, ("kv", "tp")),
        P(("grp", "dp"), KV, "tp", None, None),
        P(("grp", "dp"), None, KV, "tp", None),
        P(("grp", "dp"), None, "tp", None),
        P(("grp", "dp"), None, "tp", None),
        P(("grp", "dp"), None),
        P(("grp", "dp")),
        P(("grp", "dp"), None, KV, "tp"),
    )
    return jax.shard_map(
        shards,
        mesh=mesh,
        in_specs=placed,
        out_specs=P(("grp", "dp"), None, ("kv", "tp")),
        check_vma=False,
    )
```

```python
import functools

import jax
import jax.numpy as jnp
from jax import lax
from jax.experimental import pallas as pl
from jax.experimental.pallas import tpu as pltpu
from jax.sharding import PartitionSpec as P

D = 2048
HG = 32
G = 2
HD = 64
N = 128
CONV = 4
WIN = 7
PROP = 4
PREV = 4

KV = "kv"

INTERPRET = False


def vmem(count):
    return [pl.BlockSpec(memory_space=pltpu.VMEM)] * count


def in_vmem(x):
    return x if INTERPRET else pltpu.with_memory_space_constraint(x, pltpu.VMEM)


def in_hbm(x):
    return x if INTERPRET else pltpu.with_memory_space_constraint(x, pltpu.HBM)


def hbm(count):
    return [pl.BlockSpec(memory_space=pltpu.HBM)] * count


def pack_kernel(rows_ref, out_ref, wide):
    seqs = rows_ref.shape[0]
    for j in range(PROP):
        wide[j] = rows_ref[:, j, :].astype(jnp.float32)
    packed = jnp.concatenate(
        [
            jnp.concatenate([wide[0], wide[1]], axis=0),
            jnp.concatenate([wide[2], wide[3]], axis=0),
        ],
        axis=1,
    ).astype(jnp.bfloat16)
    for copy in range(out_ref.shape[0]):
        out_ref[copy] = packed


def places(seqs):
    at, row = {}, 0
    sizes = (("taps", 16), ("heads", 8), ("fading", PROP * seqs), ("end", 0))
    for name, size in sizes:
        at[name] = row
        row += size
    return at


def prep_kernel(*refs):
    count = 13
    sources, held, sems = refs[:count], refs[count + 3 : -1], refs[-1]
    wide_out, narrow_out, recent_out = refs[count : count + 3]
    copies = [pltpu.make_async_copy(sources[k], held[k], sems.at[k]) for k in range(count)]
    for copy in copies:
        copy.start()
    (
        gain_ref,
        dt_ref,
        mem_x_ref,
        mem_b_ref,
        mem_c_ref,
        taps_x_ref,
        taps_b_ref,
        taps_c_ref,
        heads_ref,
        parents_ref,
        admitted_ref,
        fading_ref,
        state_ref,
    ) = held
    f32 = jnp.float32
    seqs = state_ref.shape[0]
    at = places(seqs)
    for copy in copies[:-1]:
        copy.wait()
    def put(name, index, value):
        start = at[name] + index * value.shape[0]
        wide_out[start : start + value.shape[0], :] = value

    for k in range(D // N):
        pair = [
            jnp.broadcast_to(dt_ref[h : h + 1, k * N : (k + 1) * N].astype(f32), (8, N))
            for h in range(2)
        ]
        row = (k % 8) * 16
        narrow_out[seqs + k // 8, row : row + 16, :] = jnp.concatenate(pair, axis=0).astype(
            jnp.bfloat16
        )
    gains = [gain_ref[:, k * N : (k + 1) * N].astype(f32) for k in range(D // N)]
    narrow_out[seqs + D // N // 8, : D // N, :] = jnp.concatenate(gains, axis=0).astype(jnp.bfloat16)
    for t in range(CONV):
        put("taps", t, jnp.concatenate([taps_x_ref[t, h] for h in range(2)], axis=1))
        put("taps", CONV + t, taps_b_ref[t])
        put("taps", 2 * CONV + t, taps_c_ref[t])
    one = lax.broadcasted_iota(jnp.int32, (1, 2 * HD), 1) < HD
    heads = heads_ref[...]
    for place in range(3):
        row = jnp.where(one, heads[place : place + 1, 0:1], heads[place : place + 1, 1:2])
        put("heads", place, -jnp.exp(row) if place == 1 else row)

    def turned(lines):
        total = sum(line.shape[0] for line in lines)
        if total < 8:
            lines = lines + [jnp.zeros((8 - total, seqs), f32)]
        lines = jnp.concatenate(lines, axis=0)
        lines = jnp.concatenate([lines, jnp.zeros((8, N - seqs), f32)], axis=1)
        return jnp.transpose(lines)[:seqs]

    def wide(column):
        return jnp.broadcast_to(column, (seqs, 2 * HD))

    table = turned([parents_ref[...].astype(f32), admitted_ref[...].astype(f32)])
    admitted = wide(table[:, PROP : PROP + 1])
    for j in range(PROP):
        start = 3 * (CONV - 1) + j
        recent_out[start * seqs : (start + 1) * seqs, :] = wide(table[:, j : j + 1]).astype(jnp.bfloat16)
    for which, mem_ref in enumerate((mem_x_ref, mem_b_ref, mem_c_ref)):
        for back in range(CONV - 1):
            offset = CONV - 2 - back
            value = mem_ref[offset].astype(f32)
            for step in range(1, PREV + 1):
                value = jnp.where(admitted == step, mem_ref[offset + step].astype(f32), value)
            start = which * (CONV - 1) + back
            recent_out[start * seqs : (start + 1) * seqs, :] = value.astype(jnp.bfloat16)
    fading = turned([fading_ref[j, h] for j in range(PROP) for h in range(2)])
    first_head = lax.broadcasted_iota(jnp.int32, (seqs, 2 * HD), 1) < HD
    for j in range(PROP):
        pair = [wide(fading[:, 2 * j + h : 2 * j + h + 1]) for h in range(2)]
        put("fading", j, jnp.where(first_head, *pair))
    copies[-1].wait()
    narrow_out[:seqs] = state_ref[...].astype(jnp.bfloat16)


def mixer_kernel(
    pieces_ref,
    wx_ref,
    wz_far,
    wb_far,
    wc_ref,
    narrow_ref,
    wide_far,
    recent_far,
    out_ref,
    cc_all,
    read_all,
    wide_ref,
    recent_ref,
    wz_ref,
    wb_ref,
    sems,
):
    half = pieces_ref.shape[2]
    seqs = half // 2
    rows = 2 * half
    kv_count = pieces_ref.shape[1]
    f32 = jnp.float32
    copies = [
        pltpu.make_async_copy(wide_far, wide_ref, sems.at[0]),
        pltpu.make_async_copy(recent_far, recent_ref, sems.at[1]),
        pltpu.make_async_copy(wb_far, wb_ref, sems.at[2]),
        pltpu.make_async_copy(wz_far, wz_ref, sems.at[3]),
    ]
    for copy in copies:
        copy.start()
    left = lax.broadcasted_iota(jnp.int32, (half, 2 * HD), 1) < HD
    at = places(seqs)

    def table(name, index, size):
        return wide_ref[at[name] + index * size : at[name] + (index + 1) * size, :]

    gains = narrow_ref[seqs + D // N // 8, : D // N, :].astype(f32)
    scaled = []
    square = jnp.zeros((rows, 2 * HD), f32)
    for k in range(kv_count):
        p0 = pieces_ref[0, k].astype(f32)
        p1 = pieces_ref[1, k].astype(f32)
        top = jnp.where(left, p0, pltpu.roll(p1, HD, 1))
        low = jnp.where(left, pltpu.roll(p0, HD, 1), p1)
        both = jnp.concatenate([top, low], axis=0)
        square = square + both * both
        gain = gains[k : k + 1, :]
        scaled.append((both * gain).astype(jnp.bfloat16))
    u = jnp.concatenate(scaled, axis=1)
    r_in = lax.rsqrt(jnp.sum(square, axis=1, keepdims=True) / D + 1e-06)

    def times(weight, dims):
        return lax.dot_general(u, weight, dims, preferred_element_type=f32) * r_in

    across = (((1,), (1,)), ((), ()))
    down = (((1,), (0,)), ((), ()))
    c_rows = times(wc_ref[...], down).astype(jnp.bfloat16).astype(f32)
    x_rows = times(wx_ref[...], across).astype(jnp.bfloat16).astype(f32)
    chunks = [narrow_ref[seqs + k // 8, (k % 8) * 16 : (k % 8) * 16 + 16, :] for k in range(D // N)]
    dt_cols = times(jnp.concatenate(chunks, axis=1), across)
    dt_raw = jnp.where(
        lax.broadcasted_iota(jnp.int32, (rows, 2 * HD), 1) < HD,
        *(jnp.broadcast_to(dt_cols[:, c : c + 1], (rows, 2 * HD)) for c in (0, 8)),
    )

    for copy in copies:
        copy.wait()
    b_rows = times(wb_ref[...], down).astype(jnp.bfloat16).astype(f32)
    z_rows = times(wz_ref[...], across).astype(jnp.bfloat16).astype(f32)

    def recent(index):
        return recent_ref[index * seqs : (index + 1) * seqs, :].astype(f32)

    parent = [recent(3 * (CONV - 1) + j) for j in range(PROP)]
    child = [[parent[j] == i for i in range(j)] for j in range(PROP)]

    def block(array, j):
        return array[j * seqs : (j + 1) * seqs]

    def conv(row_array, which):
        history = []
        outs = []
        roots = [recent(which * (CONV - 1) + back) for back in range(CONV - 1)]
        for j in range(PROP):
            inputs = [block(row_array, j)]
            for back in range(CONV - 1):
                value = roots[back]
                for i in range(j):
                    value = jnp.where(child[j][i], history[i][back], value)
                inputs.append(value)
            history.append(inputs)
            total = None
            for lag in range(CONV):
                term = table("taps", which * CONV + CONV - 1 - lag, 1) * inputs[lag]
                total = term if total is None else total + term
            outs.append(jax.nn.silu(total))
        return outs

    cc = conv(c_rows, 2)
    for j in range(PROP):
        cc_all[:, j, :] = cc[j]
        cc_all[:, PROP + j, :] = cc[j]
    for s in range(seqs):
        read_all[s] = lax.dot_general(
            cc_all[s].astype(jnp.bfloat16), narrow_ref[s], across, preferred_element_type=f32
        )
    xc = conv(x_rows, 0)
    bc = conv(b_rows, 1)

    offset, speed, bypass = (table("heads", place, 1) for place in range(3))
    level = []
    moved = []
    above = []
    for j in range(PROP):
        raw = block(dt_raw, j) + offset
        step = jnp.maximum(raw, 0.0) + jnp.log1p(jnp.exp(-jnp.abs(raw)))
        own = speed * step + table("fading", j, seqs)
        prior = jnp.zeros_like(own)
        for i in range(j):
            prior = jnp.where(child[j][i], level[i], prior)
        level.append(own + prior)
        moved.append(step * xc[j])
        line = []
        for i in range(j):
            reach = child[j][i]
            for p in range(i + 1, j):
                reach = reach | (child[j][p] & above[p][i])
            line.append(reach)
        above.append(line)
    for j in range(PROP):
        y = jnp.exp(level[j]) * read_all[:, j, :] + bypass * xc[j]
        for i in range(j + 1):
            score = jnp.sum(cc[j] * bc[i], axis=1, keepdims=True)
            if i == j:
                y = y + score * moved[i]
            else:
                fall = jnp.exp(jnp.minimum(level[j] - level[i], 0.0))
                y = y + jnp.where(above[j][i], fall * (score * moved[i]), 0.0)
        gated = (y * jax.nn.silu(block(z_rows, j))).astype(jnp.bfloat16)
        out_ref[j * seqs : (j + 1) * seqs, :] = gated


def share_of(pieces_ref, first, weight_ref):
    f32 = jnp.float32
    kv_count, rows = pieces_ref.shape[:2]
    total = jnp.zeros((rows, weight_ref.shape[1]), f32)
    square = jnp.zeros((rows, 2 * HD), f32)
    for k in range(0, kv_count, 2):
        lhs = []
        rhs = []
        for step in range(2):
            piece = pieces_ref[k + step]
            wide = piece.astype(f32)
            square = square + wide * wide
            lhs.append(piece)
            core = first if step == 0 else 1 - first
            for h in range(2):
                start = pl.multiple_of(((2 * (k + step) + h) * G + core) * HD, HD)
                rhs.append(weight_ref[pl.ds(start, HD), :])
        total = total + jnp.dot(
            jnp.concatenate(lhs, axis=1), jnp.concatenate(rhs, axis=0), preferred_element_type=f32
        )
    return total, square


def own_kernel(first_ref, pieces_ref, weight_ref, total_ref, square_ref):
    total_ref[...], square_ref[...] = share_of(pieces_ref, first_ref[0], weight_ref)


def last_kernel(first_ref, pieces_ref, weight_ref, total_ref, square_ref, out_ref, spread):
    rows = pieces_ref.shape[1]
    seqs = rows // PROP
    total, square = share_of(pieces_ref, 1 - first_ref[0], weight_ref)
    square = jnp.sum(square + square_ref[...], axis=1, keepdims=True)
    mixed = (total + total_ref[...]) * lax.rsqrt(square / (HG * G * HD) + 1e-05)
    for j in range(PROP):
        spread[:, j, :] = mixed[j * seqs : (j + 1) * seqs]
    out_ref[...] = spread[...].astype(jnp.bfloat16)


def pack(rows, copies):
    seqs = rows.shape[0]
    return pl.pallas_call(
        pack_kernel,
        out_shape=jax.ShapeDtypeStruct((copies, 2 * seqs, 2 * HD), jnp.bfloat16),
        in_specs=vmem(1),
        out_specs=vmem(1)[0],
        scratch_shapes=[pltpu.VMEM((PROP, seqs, HD), jnp.float32)],
        compiler_params=pltpu.CompilerParams(vmem_limit_bytes=8 << 20),
        interpret=INTERPRET,
        name="pack",
    )(rows)


def prep(*inputs):
    state = inputs[-1]
    seqs = state.shape[0]
    return pl.pallas_call(
        prep_kernel,
        out_shape=[
            jax.ShapeDtypeStruct((places(seqs)["end"], N), jnp.float32),
            pltpu.VMEM((seqs + D // N // 8 + 1, N, N), jnp.bfloat16),
            jax.ShapeDtypeStruct(((3 * (CONV - 1) + PROP) * seqs, N), jnp.bfloat16),
        ],
        in_specs=[pl.BlockSpec(memory_space=pltpu.HBM)] * len(inputs),
        out_specs=vmem(3),
        scratch_shapes=[pltpu.VMEM(x.shape, x.dtype) for x in inputs]
        + [pltpu.SemaphoreType.DMA((len(inputs),))],
        compiler_params=pltpu.CompilerParams(vmem_limit_bytes=16 << 20),
        cost_estimate=pl.CostEstimate(flops=1 << 24, bytes_accessed=4 << 20, transcendentals=0),
        interpret=INTERPRET,
        name="prep",
    )(*(in_hbm(x) for x in inputs))


def mixer(pieces, *rest):
    half = pieces.shape[2]
    return pl.pallas_call(
        mixer_kernel,
        out_shape=jax.ShapeDtypeStruct((2 * half, 2 * HD), jnp.bfloat16),
        in_specs=vmem(2) + hbm(2) + vmem(2) + hbm(2),
        out_specs=vmem(1)[0],
        scratch_shapes=[
            pltpu.VMEM((half // 2, 2 * PROP, N), jnp.float32),
            pltpu.VMEM((half // 2, 2 * PROP, 2 * HD), jnp.float32),
            *(pltpu.VMEM(x.shape, x.dtype) for x in (rest[-2], rest[-1], rest[1], rest[2])),
            pltpu.SemaphoreType.DMA((4,)),
        ],
        compiler_params=pltpu.CompilerParams(vmem_limit_bytes=20 << 20),
        cost_estimate=pl.CostEstimate(
            flops=2 * 2 * half * D * 5 * N, bytes_accessed=5 << 20, transcendentals=2 * half * 1000
        ),
        interpret=INTERPRET,
        name="mixer",
    )(pieces, *rest)


def cost_of(pieces, weight):
    kv_count, rows, width = pieces.shape
    return pl.CostEstimate(
        flops=2 * rows * kv_count * width * weight.shape[1], bytes_accessed=1 << 20, transcendentals=rows
    )


def own_half(first, pieces, weight):
    rows = pieces.shape[1]
    return pl.pallas_call(
        own_kernel,
        out_shape=[
            jax.ShapeDtypeStruct((rows, weight.shape[1]), jnp.float32),
            jax.ShapeDtypeStruct((rows, 2 * HD), jnp.float32),
        ],
        in_specs=[pl.BlockSpec(memory_space=pltpu.SMEM)] + vmem(2),
        out_specs=vmem(2),
        compiler_params=pltpu.CompilerParams(vmem_limit_bytes=16 << 20),
        cost_estimate=cost_of(pieces, weight),
        interpret=INTERPRET,
        name="own_half",
    )(first, pieces, weight)


def last(first, pieces, weight, total, square):
    rows = pieces.shape[1]
    seqs = rows // PROP
    cols = weight.shape[1]
    return pl.pallas_call(
        last_kernel,
        out_shape=jax.ShapeDtypeStruct((seqs, PROP, cols), jnp.bfloat16),
        in_specs=[pl.BlockSpec(memory_space=pltpu.SMEM)] + vmem(4),
        out_specs=vmem(1)[0],
        scratch_shapes=[pltpu.VMEM((seqs, PROP, cols), jnp.float32)],
        compiler_params=pltpu.CompilerParams(vmem_limit_bytes=16 << 20),
        cost_estimate=cost_of(pieces, weight),
        interpret=INTERPRET,
        name="last",
    )(first, pieces, weight, total, square)


def prepared(
    kv_index,
    tp_index,
    leading_scaling_factor,
    lane_feed_matrix,
    final_valve_matrix,
    increment_matrix,
    entry_basis_matrix,
    readout_basis_matrix,
    lane_feed_kernel,
    entry_basis_kernel,
    readout_basis_kernel,
    increment_offset,
    shrink_speed_exponent,
    lane_bypass_factor,
    hidden_carried_memory,
    lane_filter_memory,
    entry_basis_memory,
    readout_basis_memory,
    predecessor_index,
    admitted_counts,
    surplus_fading,
):
    seqs = predecessor_index.shape[0]
    heads = increment_offset.shape[0]
    wx = jnp.transpose(lane_feed_matrix, (1, 2, 3, 0)).reshape(heads * HD, D)
    wz = jnp.transpose(final_valve_matrix, (1, 2, 3, 0)).reshape(heads * HD, D)
    dt_own = lax.dynamic_slice(
        jnp.transpose(increment_matrix, (1, 2, 0)), (kv_index * heads, tp_index, 0), (heads, 1, D)
    )
    wb = entry_basis_matrix.reshape(D, N)
    wc = readout_basis_matrix.reshape(D, N)
    head_rows = jnp.stack(
        [x.reshape(heads) for x in (increment_offset, shrink_speed_exponent, lane_bypass_factor)]
    )
    wide, narrow, recent = prep(
        leading_scaling_factor.reshape(1, D),
        dt_own.reshape(heads, D),
        jnp.transpose(lane_filter_memory, (1, 0, 2, 3, 4)).reshape(WIN, seqs, heads * HD),
        jnp.transpose(entry_basis_memory, (1, 0, 2, 3)).reshape(WIN, seqs, N),
        jnp.transpose(readout_basis_memory, (1, 0, 2, 3)).reshape(WIN, seqs, N),
        lane_feed_kernel,
        entry_basis_kernel,
        readout_basis_kernel,
        head_rows,
        jnp.transpose(predecessor_index),
        admitted_counts.reshape(1, seqs),
        jnp.transpose(surplus_fading, (1, 2, 3, 0)),
        hidden_carried_memory.reshape(seqs, heads * HD, N),
    )
    return (wx, in_hbm(wz), in_hbm(wb), wc, in_vmem(narrow), in_hbm(wide), in_hbm(recent))


def shards(candidate_vectors, leading_scaling_factor, lane_feed_matrix, final_valve_matrix,
           increment_matrix, entry_basis_matrix, readout_basis_matrix, lane_feed_kernel,
           entry_basis_kernel, readout_basis_kernel, increment_offset, shrink_speed_exponent,
           lane_bypass_factor, final_linear_matrix, *memories):
    copies = pack(candidate_vectors, lax.axis_size(KV))
    along = lax.all_to_all(copies, KV, split_axis=0, concat_axis=0, tiled=True)
    pieces = lax.all_gather(along, "tp")
    rest = prepared(
        lax.axis_index(KV), lax.axis_index("tp"), leading_scaling_factor, lane_feed_matrix,
        final_valve_matrix, increment_matrix, entry_basis_matrix, readout_basis_matrix,
        lane_feed_kernel, entry_basis_kernel, readout_basis_kernel, increment_offset,
        shrink_speed_exponent, lane_bypass_factor, *memories,
    )
    gated = mixer(pieces, *rest)
    rings = [[G * z + (z + t) % G for z in range(lax.axis_size(KV))] for t in range(G)]
    along = lax.all_gather(gated, (KV, "tp"), axis_index_groups=rings)
    swapped = lax.ppermute(along, "tp", [(0, 1), (1, 0)])
    weight = final_linear_matrix.reshape(HG * G * HD, -1)
    first = ((lax.axis_index(KV) + lax.axis_index("tp")) % G).reshape(1)
    return last(first, swapped, weight, *own_half(first, along, weight))


def solution(mesh):
    placed = (
        P(("grp", "dp"), None, ("kv", "tp")),
        P(),
        P(None, KV, "tp", None),
        P(None, KV, "tp", None),
        P(),
        P(None, "tp", None),
        P(None, "tp", None),
        P(None, KV, "tp", None),
        P(None, "tp", None),
        P(None, "tp", None),
        P(KV, "tp"),
        P(KV, "tp"),
        P(KV, "tp"),
        P(None, None, None, ("kv", "tp")),
        P(("grp", "dp"), KV, "tp", None, None),
        P(("grp", "dp"), None, KV, "tp", None),
        P(("grp", "dp"), None, "tp", None),
        P(("grp", "dp"), None, "tp", None),
        P(("grp", "dp"), None),
        P(("grp", "dp")),
        P(("grp", "dp"), None, KV, "tp"),
    )
    return jax.shard_map(
        shards,
        mesh=mesh,
        in_specs=placed,
        out_specs=P(("grp", "dp"), None, ("kv", "tp")),
        check_vma=False,
    )
```

```python
import functools

import jax
import jax.numpy as jnp
from jax import lax
from jax.experimental import pallas as pl
from jax.experimental.pallas import tpu as pltpu
from jax.sharding import PartitionSpec as P

D = 2048
HG = 32
G = 2
HD = 64
N = 128
CONV = 4
WIN = 7
PROP = 4
PREV = 4

KV = "kv"

INTERPRET = False


def vmem(count):
    return [pl.BlockSpec(memory_space=pltpu.VMEM)] * count


def in_vmem(x):
    return x if INTERPRET else pltpu.with_memory_space_constraint(x, pltpu.VMEM)


def in_hbm(x):
    return x if INTERPRET else pltpu.with_memory_space_constraint(x, pltpu.HBM)


def hbm(count):
    return [pl.BlockSpec(memory_space=pltpu.HBM)] * count


def pack_kernel(rows_ref, out_ref, wide):
    seqs = rows_ref.shape[0]
    for j in range(PROP):
        wide[j] = rows_ref[:, j, :].astype(jnp.float32)
    packed = jnp.concatenate(
        [
            jnp.concatenate([wide[0], wide[1]], axis=0),
            jnp.concatenate([wide[2], wide[3]], axis=0),
        ],
        axis=1,
    ).astype(jnp.bfloat16)
    for copy in range(out_ref.shape[0]):
        out_ref[copy] = packed


def places(seqs):
    at, row = {}, 0
    sizes = (("state", seqs * N), ("dt", 16 * (D // N)), ("recent", 3 * (CONV - 1) * seqs))
    sizes += (("parent", PROP * seqs), ("gain", D // N))
    for part in range(3):
        sizes += ((f"taps{part}", 16), (f"heads{part}", 16), (f"fading{part}", PROP * seqs))
    for name, size in (*sizes, ("end", 0)):
        at[name] = row
        row += size
    return at


def prep_kernel(*refs):
    count = 13
    sources, all_out, held, sems = refs[:count], refs[count], refs[count + 1 : -1], refs[-1]
    copies = [pltpu.make_async_copy(sources[k], held[k], sems.at[k]) for k in range(count)]
    for copy in copies:
        copy.start()
    (
        gain_ref,
        dt_ref,
        mem_x_ref,
        mem_b_ref,
        mem_c_ref,
        taps_x_ref,
        taps_b_ref,
        taps_c_ref,
        heads_ref,
        parents_ref,
        admitted_ref,
        fading_ref,
        state_ref,
    ) = held
    f32 = jnp.float32
    seqs = state_ref.shape[0]
    at = places(seqs)
    for copy in copies[:-1]:
        copy.wait()
    def put(name, index, value):
        start = at[name] + index * value.shape[0]
        all_out[start : start + value.shape[0], :] = value.astype(jnp.bfloat16)

    def put_parts(name, index, value):
        for part in range(3):
            put(f"{name}{part}", index, value)
            value = value - value.astype(jnp.bfloat16).astype(f32)

    def rows_of(lines):
        return jnp.concatenate(lines + [jnp.zeros((16 - len(lines), N), f32)], axis=0)

    for k in range(D // N):
        pair = [
            jnp.broadcast_to(dt_ref[h : h + 1, k * N : (k + 1) * N].astype(f32), (8, N))
            for h in range(2)
        ]
        put("dt", k, jnp.concatenate(pair, axis=0))
    gains = [gain_ref[:, k * N : (k + 1) * N].astype(f32) for k in range(D // N)]
    put("gain", 0, jnp.concatenate(gains, axis=0))
    taps = [jnp.concatenate([taps_x_ref[t, h] for h in range(2)], axis=1) for t in range(CONV)]
    taps += [taps_b_ref[t] for t in range(CONV)] + [taps_c_ref[t] for t in range(CONV)]
    put_parts("taps", 0, rows_of(taps))
    one = lax.broadcasted_iota(jnp.int32, (1, 2 * HD), 1) < HD
    heads = heads_ref[...]
    lines = [
        jnp.where(one, heads[place : place + 1, 0:1], heads[place : place + 1, 1:2])
        for place in range(3)
    ]
    put_parts("heads", 0, rows_of([lines[0], -jnp.exp(lines[1]), lines[2]]))

    def turned(lines):
        total = sum(line.shape[0] for line in lines)
        if total < 8:
            lines = lines + [jnp.zeros((8 - total, seqs), f32)]
        lines = jnp.concatenate(lines, axis=0)
        lines = jnp.concatenate([lines, jnp.zeros((8, N - seqs), f32)], axis=1)
        return jnp.transpose(lines)[:seqs]

    def wide(column):
        return jnp.broadcast_to(column, (seqs, 2 * HD))

    table = turned([parents_ref[...].astype(f32), admitted_ref[...].astype(f32)])
    admitted = wide(table[:, PROP : PROP + 1])
    for j in range(PROP):
        put("parent", j, wide(table[:, j : j + 1]))
    for which, mem_ref in enumerate((mem_x_ref, mem_b_ref, mem_c_ref)):
        for back in range(CONV - 1):
            offset = CONV - 2 - back
            value = mem_ref[offset].astype(f32)
            for step in range(1, PREV + 1):
                value = jnp.where(admitted == step, mem_ref[offset + step].astype(f32), value)
            put("recent", which * (CONV - 1) + back, value)
    fading = turned([fading_ref[j, h] for j in range(PROP) for h in range(2)])
    first_head = lax.broadcasted_iota(jnp.int32, (seqs, 2 * HD), 1) < HD
    for j in range(PROP):
        pair = [wide(fading[:, 2 * j + h : 2 * j + h + 1]) for h in range(2)]
        put_parts("fading", j, jnp.where(first_head, *pair))
    copies[-1].wait()
    all_out[: seqs * N, :] = state_ref[...].reshape(seqs * N, N).astype(jnp.bfloat16)


def mixer_kernel(
    pieces_ref,
    wx_ref,
    wz_far,
    wb_far,
    wc_far,
    tables_ref,
    out_ref,
    cc_all,
    read_all,
    wc_ref,
    wb_ref,
    wz_ref,
    sems,
):
    half = pieces_ref.shape[2]
    seqs = half // 2
    rows = 2 * half
    kv_count = pieces_ref.shape[1]
    f32 = jnp.float32
    wc_copy = pltpu.make_async_copy(wc_far, wc_ref, sems.at[0])
    wb_copy = pltpu.make_async_copy(wb_far, wb_ref, sems.at[1])
    wz_copy = pltpu.make_async_copy(wz_far, wz_ref, sems.at[2])
    wc_copy.start()
    wb_copy.start()
    wz_copy.start()
    left = lax.broadcasted_iota(jnp.int32, (half, 2 * HD), 1) < HD
    at = places(seqs)

    def table(name, index, size):
        return tables_ref[at[name] + index * size : at[name] + (index + 1) * size, :].astype(f32)

    def whole(name, index, size):
        high, middle, low = (table(f"{name}{part}", index, size) for part in range(3))
        return high + middle + low

    gains = table("gain", 0, D // N)
    taps = whole("taps", 0, 16)
    heads = whole("heads", 0, 16)
    scaled = []
    square = jnp.zeros((rows, 2 * HD), f32)
    for k in range(kv_count):
        p0 = pieces_ref[0, k].astype(f32)
        p1 = pieces_ref[1, k].astype(f32)
        top = jnp.where(left, p0, pltpu.roll(p1, HD, 1))
        low = jnp.where(left, pltpu.roll(p0, HD, 1), p1)
        both = jnp.concatenate([top, low], axis=0)
        square = square + both * both
        gain = gains[k : k + 1, :]
        scaled.append((both * gain).astype(jnp.bfloat16))
    u = jnp.concatenate(scaled, axis=1)
    r_in = lax.rsqrt(jnp.sum(square, axis=1, keepdims=True) / D + 1e-06)

    def times(weight, dims):
        return lax.dot_general(u, weight, dims, preferred_element_type=f32) * r_in

    across = (((1,), (1,)), ((), ()))
    down = (((1,), (0,)), ((), ()))
    x_rows = times(wx_ref[...], across).astype(jnp.bfloat16).astype(f32)
    chunks = [tables_ref[at["dt"] + 16 * k : at["dt"] + 16 * (k + 1), :] for k in range(D // N)]
    dt_cols = times(jnp.concatenate(chunks, axis=1), across)
    dt_raw = jnp.where(
        lax.broadcasted_iota(jnp.int32, (rows, 2 * HD), 1) < HD,
        *(jnp.broadcast_to(dt_cols[:, c : c + 1], (rows, 2 * HD)) for c in (0, 8)),
    )


    parent = [table("parent", j, seqs) for j in range(PROP)]
    child = [[parent[j] == i for i in range(j)] for j in range(PROP)]

    def block(array, j):
        return array[j * seqs : (j + 1) * seqs]

    def conv(row_array, which):
        history = []
        outs = []
        roots = [table("recent", which * (CONV - 1) + back, seqs) for back in range(CONV - 1)]
        for j in range(PROP):
            inputs = [block(row_array, j)]
            for back in range(CONV - 1):
                value = roots[back]
                for i in range(j):
                    value = jnp.where(child[j][i], history[i][back], value)
                inputs.append(value)
            history.append(inputs)
            total = None
            for lag in range(CONV):
                place = which * CONV + CONV - 1 - lag
                term = taps[place : place + 1, :] * inputs[lag]
                total = term if total is None else total + term
            outs.append(jax.nn.silu(total))
        return outs

    xc = conv(x_rows, 0)

    offset, speed, bypass = (heads[place : place + 1, :] for place in range(3))
    level = []
    moved = []
    above = []
    for j in range(PROP):
        raw = block(dt_raw, j) + offset
        step = jnp.maximum(raw, 0.0) + jnp.log1p(jnp.exp(-jnp.abs(raw)))
        own = speed * step + whole("fading", j, seqs)
        prior = jnp.zeros_like(own)
        for i in range(j):
            prior = jnp.where(child[j][i], level[i], prior)
        level.append(own + prior)
        moved.append(step * xc[j])
        line = []
        for i in range(j):
            reach = child[j][i]
            for p in range(i + 1, j):
                reach = reach | (child[j][p] & above[p][i])
            line.append(reach)
        above.append(line)
    wc_copy.wait()
    c_rows = times(wc_ref[...], down).astype(jnp.bfloat16).astype(f32)
    cc = conv(c_rows, 2)
    for j in range(PROP):
        cc_all[:, j, :] = cc[j]
        cc_all[:, PROP + j, :] = cc[j]
    for s in range(seqs):
        read_all[s] = lax.dot_general(
            cc_all[s].astype(jnp.bfloat16),
            tables_ref[s * N : (s + 1) * N, :],
            across,
            preferred_element_type=f32,
        )
    wb_copy.wait()
    b_rows = times(wb_ref[...], down).astype(jnp.bfloat16).astype(f32)
    bc = conv(b_rows, 1)
    inner = []
    for j in range(PROP):
        y = bypass * xc[j]
        for i in range(j + 1):
            score = jnp.sum(cc[j] * bc[i], axis=1, keepdims=True)
            if i == j:
                y = y + score * moved[i]
            else:
                fall = jnp.exp(jnp.minimum(level[j] - level[i], 0.0))
                y = y + jnp.where(above[j][i], fall * (score * moved[i]), 0.0)
        inner.append(y)
    outs = [jnp.exp(level[j]) * read_all[:, j, :] + inner[j] for j in range(PROP)]
    wz_copy.wait()
    z_rows = times(wz_ref[...], across).astype(jnp.bfloat16).astype(f32)
    for j in range(PROP):
        gated = outs[j] * jax.nn.silu(block(z_rows, j))
        out_ref[j * seqs : (j + 1) * seqs, :] = gated.astype(jnp.bfloat16)


def share_of(pieces_ref, first, weight_ref):
    f32 = jnp.float32
    kv_count, rows = pieces_ref.shape[:2]
    total = jnp.zeros((rows, weight_ref.shape[1]), f32)
    square = jnp.zeros((rows, 2 * HD), f32)
    for k in range(0, kv_count, 2):
        lhs = []
        rhs = []
        for step in range(2):
            piece = pieces_ref[k + step]
            wide = piece.astype(f32)
            square = square + wide * wide
            lhs.append(piece)
            core = first if step == 0 else 1 - first
            for h in range(2):
                start = pl.multiple_of(((2 * (k + step) + h) * G + core) * HD, HD)
                rhs.append(weight_ref[pl.ds(start, HD), :])
        total = total + jnp.dot(
            jnp.concatenate(lhs, axis=1), jnp.concatenate(rhs, axis=0), preferred_element_type=f32
        )
    return total, square


def own_kernel(first_ref, pieces_ref, weight_ref, total_ref, square_ref):
    total_ref[...], square_ref[...] = share_of(pieces_ref, first_ref[0], weight_ref)


def last_kernel(first_ref, pieces_ref, weight_ref, total_ref, square_ref, out_ref, spread):
    rows = pieces_ref.shape[1]
    seqs = rows // PROP
    total, square = share_of(pieces_ref, 1 - first_ref[0], weight_ref)
    square = jnp.sum(square + square_ref[...], axis=1, keepdims=True)
    mixed = (total + total_ref[...]) * lax.rsqrt(square / (HG * G * HD) + 1e-05)
    for j in range(PROP):
        spread[:, j, :] = mixed[j * seqs : (j + 1) * seqs]
    out_ref[...] = spread[...].astype(jnp.bfloat16)


def pack(rows, copies):
    seqs = rows.shape[0]
    return pl.pallas_call(
        pack_kernel,
        out_shape=jax.ShapeDtypeStruct((copies, 2 * seqs, 2 * HD), jnp.bfloat16),
        in_specs=vmem(1),
        out_specs=vmem(1)[0],
        scratch_shapes=[pltpu.VMEM((PROP, seqs, HD), jnp.float32)],
        compiler_params=pltpu.CompilerParams(vmem_limit_bytes=8 << 20),
        interpret=INTERPRET,
        name="pack",
    )(rows)


def prep(*inputs):
    state = inputs[-1]
    seqs = state.shape[0]
    return pl.pallas_call(
        prep_kernel,
        out_shape=pltpu.VMEM((places(seqs)["end"], N), jnp.bfloat16),
        in_specs=[pl.BlockSpec(memory_space=pltpu.HBM)] * len(inputs),
        out_specs=vmem(1)[0],
        scratch_shapes=[pltpu.VMEM(x.shape, x.dtype) for x in inputs]
        + [pltpu.SemaphoreType.DMA((len(inputs),))],
        compiler_params=pltpu.CompilerParams(vmem_limit_bytes=16 << 20),
        cost_estimate=pl.CostEstimate(flops=1 << 24, bytes_accessed=4 << 20, transcendentals=0),
        interpret=INTERPRET,
        name="prep",
    )(*(in_hbm(x) for x in inputs))


def mixer(pieces, *rest):
    half = pieces.shape[2]
    return pl.pallas_call(
        mixer_kernel,
        out_shape=jax.ShapeDtypeStruct((2 * half, 2 * HD), jnp.bfloat16),
        in_specs=vmem(2) + hbm(3) + vmem(1),
        out_specs=vmem(1)[0],
        scratch_shapes=[
            pltpu.VMEM((half // 2, 2 * PROP, N), jnp.float32),
            pltpu.VMEM((half // 2, 2 * PROP, 2 * HD), jnp.float32),
            *(pltpu.VMEM(x.shape, x.dtype) for x in (rest[3], rest[2], rest[1])),
            pltpu.SemaphoreType.DMA((3,)),
        ],
        compiler_params=pltpu.CompilerParams(vmem_limit_bytes=20 << 20),
        cost_estimate=pl.CostEstimate(
            flops=2 * 2 * half * D * 5 * N, bytes_accessed=5 << 20, transcendentals=2 * half * 1000
        ),
        interpret=INTERPRET,
        name="mixer",
    )(pieces, *rest)


def cost_of(pieces, weight):
    kv_count, rows, width = pieces.shape
    return pl.CostEstimate(
        flops=2 * rows * kv_count * width * weight.shape[1], bytes_accessed=1 << 20, transcendentals=rows
    )


def own_half(first, pieces, weight):
    rows = pieces.shape[1]
    return pl.pallas_call(
        own_kernel,
        out_shape=[
            jax.ShapeDtypeStruct((rows, weight.shape[1]), jnp.float32),
            jax.ShapeDtypeStruct((rows, 2 * HD), jnp.float32),
        ],
        in_specs=[pl.BlockSpec(memory_space=pltpu.SMEM)] + vmem(2),
        out_specs=vmem(2),
        compiler_params=pltpu.CompilerParams(vmem_limit_bytes=16 << 20),
        cost_estimate=cost_of(pieces, weight),
        interpret=INTERPRET,
        name="own_half",
    )(first, pieces, weight)


def last(first, pieces, weight, total, square):
    rows = pieces.shape[1]
    seqs = rows // PROP
    cols = weight.shape[1]
    return pl.pallas_call(
        last_kernel,
        out_shape=jax.ShapeDtypeStruct((seqs, PROP, cols), jnp.bfloat16),
        in_specs=[pl.BlockSpec(memory_space=pltpu.SMEM)] + vmem(4),
        out_specs=vmem(1)[0],
        scratch_shapes=[pltpu.VMEM((seqs, PROP, cols), jnp.float32)],
        compiler_params=pltpu.CompilerParams(vmem_limit_bytes=16 << 20),
        cost_estimate=cost_of(pieces, weight),
        interpret=INTERPRET,
        name="last",
    )(first, pieces, weight, total, square)


def prepared(
    kv_index,
    tp_index,
    leading_scaling_factor,
    lane_feed_matrix,
    final_valve_matrix,
    increment_matrix,
    entry_basis_matrix,
    readout_basis_matrix,
    lane_feed_kernel,
    entry_basis_kernel,
    readout_basis_kernel,
    increment_offset,
    shrink_speed_exponent,
    lane_bypass_factor,
    hidden_carried_memory,
    lane_filter_memory,
    entry_basis_memory,
    readout_basis_memory,
    predecessor_index,
    admitted_counts,
    surplus_fading,
):
    seqs = predecessor_index.shape[0]
    heads = increment_offset.shape[0]
    wx = jnp.transpose(lane_feed_matrix, (1, 2, 3, 0)).reshape(heads * HD, D)
    wz = jnp.transpose(final_valve_matrix, (1, 2, 3, 0)).reshape(heads * HD, D)
    dt_own = lax.dynamic_slice(
        jnp.transpose(increment_matrix, (1, 2, 0)), (kv_index * heads, tp_index, 0), (heads, 1, D)
    )
    wb = entry_basis_matrix.reshape(D, N)
    wc = readout_basis_matrix.reshape(D, N)
    head_rows = jnp.stack(
        [x.reshape(heads) for x in (increment_offset, shrink_speed_exponent, lane_bypass_factor)]
    )
    tables = prep(
        leading_scaling_factor.reshape(1, D),
        dt_own.reshape(heads, D),
        jnp.transpose(lane_filter_memory, (1, 0, 2, 3, 4)).reshape(WIN, seqs, heads * HD),
        jnp.transpose(entry_basis_memory, (1, 0, 2, 3)).reshape(WIN, seqs, N),
        jnp.transpose(readout_basis_memory, (1, 0, 2, 3)).reshape(WIN, seqs, N),
        lane_feed_kernel,
        entry_basis_kernel,
        readout_basis_kernel,
        head_rows,
        jnp.transpose(predecessor_index),
        admitted_counts.reshape(1, seqs),
        jnp.transpose(surplus_fading, (1, 2, 3, 0)),
        hidden_carried_memory.reshape(seqs, heads * HD, N),
    )
    return (wx, in_hbm(wz), in_hbm(wb), in_hbm(wc), in_vmem(tables))


def shards(candidate_vectors, leading_scaling_factor, lane_feed_matrix, final_valve_matrix,
           increment_matrix, entry_basis_matrix, readout_basis_matrix, lane_feed_kernel,
           entry_basis_kernel, readout_basis_kernel, increment_offset, shrink_speed_exponent,
           lane_bypass_factor, final_linear_matrix, *memories):
    copies = pack(candidate_vectors, lax.axis_size(KV))
    along = lax.all_to_all(copies, KV, split_axis=0, concat_axis=0, tiled=True)
    pieces = lax.all_gather(along, "tp")
    rest = prepared(
        lax.axis_index(KV), lax.axis_index("tp"), leading_scaling_factor, lane_feed_matrix,
        final_valve_matrix, increment_matrix, entry_basis_matrix, readout_basis_matrix,
        lane_feed_kernel, entry_basis_kernel, readout_basis_kernel, increment_offset,
        shrink_speed_exponent, lane_bypass_factor, *memories,
    )
    gated = mixer(pieces, *rest)
    rings = [[G * z + (z + t) % G for z in range(lax.axis_size(KV))] for t in range(G)]
    along = lax.all_gather(gated, (KV, "tp"), axis_index_groups=rings)
    swapped = lax.ppermute(along, "tp", [(0, 1), (1, 0)])
    weight = final_linear_matrix.reshape(HG * G * HD, -1)
    first = ((lax.axis_index(KV) + lax.axis_index("tp")) % G).reshape(1)
    return last(first, swapped, weight, *own_half(first, along, weight))


def solution(mesh):
    placed = (
        P(("grp", "dp"), None, ("kv", "tp")),
        P(),
        P(None, KV, "tp", None),
        P(None, KV, "tp", None),
        P(),
        P(None, "tp", None),
        P(None, "tp", None),
        P(None, KV, "tp", None),
        P(None, "tp", None),
        P(None, "tp", None),
        P(KV, "tp"),
        P(KV, "tp"),
        P(KV, "tp"),
        P(None, None, None, ("kv", "tp")),
        P(("grp", "dp"), KV, "tp", None, None),
        P(("grp", "dp"), None, KV, "tp", None),
        P(("grp", "dp"), None, "tp", None),
        P(("grp", "dp"), None, "tp", None),
        P(("grp", "dp"), None),
        P(("grp", "dp")),
        P(("grp", "dp"), None, KV, "tp"),
    )
    return jax.shard_map(
        shards,
        mesh=mesh,
        in_specs=placed,
        out_specs=P(("grp", "dp"), None, ("kv", "tp")),
        check_vma=False,
    )
```

```python
import functools

import jax
import jax.numpy as jnp
from jax import lax
from jax.experimental import pallas as pl
from jax.experimental.pallas import tpu as pltpu
from jax.sharding import PartitionSpec as P

D = 2048
HG = 32
G = 2
HD = 64
N = 128
CONV = 4
WIN = 7
PROP = 4
PREV = 4

KV = "kv"

INTERPRET = False


def vmem(count):
    return [pl.BlockSpec(memory_space=pltpu.VMEM)] * count


def in_vmem(x):
    return x if INTERPRET else pltpu.with_memory_space_constraint(x, pltpu.VMEM)


def in_hbm(x):
    return x if INTERPRET else pltpu.with_memory_space_constraint(x, pltpu.HBM)


def hbm(count):
    return [pl.BlockSpec(memory_space=pltpu.HBM)] * count


def pack_kernel(rows_ref, out_ref, wide):
    seqs = rows_ref.shape[0]
    for j in range(PROP):
        wide[j] = rows_ref[:, j, :].astype(jnp.float32)
    packed = jnp.concatenate(
        [
            jnp.concatenate([wide[0], wide[1]], axis=0),
            jnp.concatenate([wide[2], wide[3]], axis=0),
        ],
        axis=1,
    ).astype(jnp.bfloat16)
    for copy in range(out_ref.shape[0]):
        out_ref[copy] = packed


def places(seqs):
    at, row = {}, 0
    sizes = (("state", seqs * N), ("dt", 16 * (D // N)), ("recent", 3 * (CONV - 1) * seqs))
    sizes += (("parent", PROP * seqs), ("gain", D // N))
    for part in range(3):
        sizes += ((f"taps{part}", 16), (f"heads{part}", 16), (f"fading{part}", PROP * seqs))
    for name, size in (*sizes, ("end", 0)):
        at[name] = row
        row += size
    return at


def prep_kernel(*refs):
    count = 13
    sources, all_out, held, sems = refs[:count], refs[count], refs[count + 1 : -1], refs[-1]
    copies = [pltpu.make_async_copy(sources[k], held[k], sems.at[k]) for k in range(count)]
    for copy in copies:
        copy.start()
    (
        gain_ref,
        dt_ref,
        mem_x_ref,
        mem_b_ref,
        mem_c_ref,
        taps_x_ref,
        taps_b_ref,
        taps_c_ref,
        heads_ref,
        parents_ref,
        admitted_ref,
        fading_ref,
        state_ref,
    ) = held
    f32 = jnp.float32
    seqs = state_ref.shape[0]
    at = places(seqs)
    for copy in copies[:-1]:
        copy.wait()
    def put(name, index, value):
        start = at[name] + index * value.shape[0]
        all_out[start : start + value.shape[0], :] = value.astype(jnp.bfloat16)

    def put_parts(name, index, value):
        for part in range(3):
            put(f"{name}{part}", index, value)
            value = value - value.astype(jnp.bfloat16).astype(f32)

    def rows_of(lines):
        return jnp.concatenate(lines + [jnp.zeros((16 - len(lines), N), f32)], axis=0)

    for k in range(D // N):
        pair = [
            jnp.broadcast_to(dt_ref[h : h + 1, k * N : (k + 1) * N].astype(f32), (8, N))
            for h in range(2)
        ]
        put("dt", k, jnp.concatenate(pair, axis=0))
    gains = [gain_ref[:, k * N : (k + 1) * N].astype(f32) for k in range(D // N)]
    put("gain", 0, jnp.concatenate(gains, axis=0))
    taps = [jnp.concatenate([taps_x_ref[t, h] for h in range(2)], axis=1) for t in range(CONV)]
    taps += [taps_b_ref[t] for t in range(CONV)] + [taps_c_ref[t] for t in range(CONV)]
    put_parts("taps", 0, rows_of(taps))
    one = lax.broadcasted_iota(jnp.int32, (1, 2 * HD), 1) < HD
    heads = heads_ref[...]
    lines = [
        jnp.where(one, heads[place : place + 1, 0:1], heads[place : place + 1, 1:2])
        for place in range(3)
    ]
    put_parts("heads", 0, rows_of([lines[0], -jnp.exp(lines[1]), lines[2]]))

    def turned(lines):
        total = sum(line.shape[0] for line in lines)
        if total < 8:
            lines = lines + [jnp.zeros((8 - total, seqs), f32)]
        lines = jnp.concatenate(lines, axis=0)
        lines = jnp.concatenate([lines, jnp.zeros((8, N - seqs), f32)], axis=1)
        return jnp.transpose(lines)[:seqs]

    def wide(column):
        return jnp.broadcast_to(column, (seqs, 2 * HD))

    table = turned([parents_ref[...].astype(f32), admitted_ref[...].astype(f32)])
    admitted = wide(table[:, PROP : PROP + 1])
    for j in range(PROP):
        put("parent", j, wide(table[:, j : j + 1]))
    for which, mem_ref in enumerate((mem_x_ref, mem_b_ref, mem_c_ref)):
        for back in range(CONV - 1):
            offset = CONV - 2 - back
            value = mem_ref[offset].astype(f32)
            for step in range(1, PREV + 1):
                value = jnp.where(admitted == step, mem_ref[offset + step].astype(f32), value)
            put("recent", which * (CONV - 1) + back, value)
    fading = turned([fading_ref[j, h] for j in range(PROP) for h in range(2)])
    first_head = lax.broadcasted_iota(jnp.int32, (seqs, 2 * HD), 1) < HD
    for j in range(PROP):
        pair = [wide(fading[:, 2 * j + h : 2 * j + h + 1]) for h in range(2)]
        put_parts("fading", j, jnp.where(first_head, *pair))
    copies[-1].wait()
    all_out[: seqs * N, :] = state_ref[...].reshape(seqs * N, N).astype(jnp.bfloat16)


def mixer_kernel(
    pieces_ref,
    wx_ref,
    wz_far,
    wb_far,
    wc_far,
    tables_ref,
    out_ref,
    cc_all,
    read_all,
    wc_ref,
    wb_ref,
    wz_ref,
    sems,
):
    half = pieces_ref.shape[2]
    seqs = half // 2
    rows = 2 * half
    kv_count = pieces_ref.shape[1]
    f32 = jnp.float32
    wc_copy = pltpu.make_async_copy(wc_far, wc_ref, sems.at[0])
    wb_copy = pltpu.make_async_copy(wb_far, wb_ref, sems.at[1])
    wz_copy = pltpu.make_async_copy(wz_far, wz_ref, sems.at[2])
    wc_copy.start()
    wb_copy.start()
    wz_copy.start()
    left = lax.broadcasted_iota(jnp.int32, (half, 2 * HD), 1) < HD
    at = places(seqs)

    def table(name, index, size):
        return tables_ref[at[name] + index * size : at[name] + (index + 1) * size, :].astype(f32)

    def whole(name, index, size):
        high, middle, low = (table(f"{name}{part}", index, size) for part in range(3))
        return high + middle + low

    gains = table("gain", 0, D // N)
    taps = whole("taps", 0, 16)
    heads = whole("heads", 0, 16)
    scaled = []
    square = jnp.zeros((rows, 2 * HD), f32)
    for k in range(kv_count):
        p0 = pieces_ref[0, k].astype(f32)
        p1 = pieces_ref[1, k].astype(f32)
        top = jnp.where(left, p0, pltpu.roll(p1, HD, 1))
        low = jnp.where(left, pltpu.roll(p0, HD, 1), p1)
        both = jnp.concatenate([top, low], axis=0)
        square = square + both * both
        gain = gains[k : k + 1, :]
        scaled.append((both * gain).astype(jnp.bfloat16))
    u = jnp.concatenate(scaled, axis=1)
    r_in = lax.rsqrt(jnp.sum(square, axis=1, keepdims=True) / D + 1e-06)

    def times(weight, dims):
        return lax.dot_general(u, weight, dims, preferred_element_type=f32) * r_in

    across = (((1,), (1,)), ((), ()))
    down = (((1,), (0,)), ((), ()))
    x_rows = times(wx_ref[...], across).astype(jnp.bfloat16).astype(f32)
    chunks = [tables_ref[at["dt"] + 16 * k : at["dt"] + 16 * (k + 1), :] for k in range(D // N)]
    dt_cols = times(jnp.concatenate(chunks, axis=1), across)
    dt_raw = jnp.where(
        lax.broadcasted_iota(jnp.int32, (rows, 2 * HD), 1) < HD,
        *(jnp.broadcast_to(dt_cols[:, c : c + 1], (rows, 2 * HD)) for c in (0, 8)),
    )


    parent = [table("parent", j, seqs) for j in range(PROP)]
    child = [[parent[j] == i for i in range(j)] for j in range(PROP)]

    def block(array, j):
        return array[j * seqs : (j + 1) * seqs]

    def conv(row_array, which):
        history = []
        outs = []
        roots = [table("recent", which * (CONV - 1) + back, seqs) for back in range(CONV - 1)]
        for j in range(PROP):
            inputs = [block(row_array, j)]
            for back in range(CONV - 1):
                value = roots[back]
                for i in range(j):
                    value = jnp.where(child[j][i], history[i][back], value)
                inputs.append(value)
            history.append(inputs)
            total = None
            for lag in range(CONV):
                place = which * CONV + CONV - 1 - lag
                term = taps[place : place + 1, :] * inputs[lag]
                total = term if total is None else total + term
            outs.append(jax.nn.silu(total))
        return outs

    xc = conv(x_rows, 0)

    offset, speed, bypass = (heads[place : place + 1, :] for place in range(3))
    level = []
    moved = []
    above = []
    for j in range(PROP):
        raw = block(dt_raw, j) + offset
        step = jnp.maximum(raw, 0.0) + jnp.log1p(jnp.exp(-jnp.abs(raw)))
        own = speed * step + whole("fading", j, seqs)
        prior = jnp.zeros_like(own)
        for i in range(j):
            prior = jnp.where(child[j][i], level[i], prior)
        level.append(own + prior)
        moved.append(step * xc[j])
        line = []
        for i in range(j):
            reach = child[j][i]
            for p in range(i + 1, j):
                reach = reach | (child[j][p] & above[p][i])
            line.append(reach)
        above.append(line)
    wc_copy.wait()
    c_rows = times(wc_ref[...], down).astype(jnp.bfloat16).astype(f32)
    cc = conv(c_rows, 2)
    for j in range(PROP):
        cc_all[:, j, :] = cc[j]
        cc_all[:, PROP + j, :] = cc[j]
    for s in range(seqs):
        read_all[s] = lax.dot_general(
            cc_all[s].astype(jnp.bfloat16),
            tables_ref[s * N : (s + 1) * N, :],
            across,
            preferred_element_type=f32,
        )
    wb_copy.wait()
    b_rows = times(wb_ref[...], down).astype(jnp.bfloat16).astype(f32)
    bc = conv(b_rows, 1)
    inner = []
    for j in range(PROP):
        y = bypass * xc[j]
        for i in range(j + 1):
            score = jnp.sum(cc[j] * bc[i], axis=1, keepdims=True)
            if i == j:
                y = y + score * moved[i]
            else:
                fall = jnp.exp(jnp.minimum(level[j] - level[i], 0.0))
                y = y + jnp.where(above[j][i], fall * (score * moved[i]), 0.0)
        inner.append(y)
    outs = [jnp.exp(level[j]) * read_all[:, j, :] + inner[j] for j in range(PROP)]
    wz_copy.wait()
    z_rows = times(wz_ref[...], across).astype(jnp.bfloat16).astype(f32)
    for j in range(PROP):
        gated = outs[j] * jax.nn.silu(block(z_rows, j))
        out_ref[j * seqs : (j + 1) * seqs, :] = gated.astype(jnp.bfloat16)


def share_of(pieces_ref, first, weight_ref):
    f32 = jnp.float32
    kv_count, rows = pieces_ref.shape[:2]
    total = jnp.zeros((rows, weight_ref.shape[1]), f32)
    square = jnp.zeros((rows, 2 * HD), f32)
    for k in range(0, kv_count, 2):
        lhs = []
        rhs = []
        for step in range(2):
            piece = pieces_ref[k + step]
            wide = piece.astype(f32)
            square = square + wide * wide
            lhs.append(piece)
            core = first if step == 0 else 1 - first
            for h in range(2):
                start = pl.multiple_of(((2 * (k + step) + h) * G + core) * HD, HD)
                rhs.append(weight_ref[pl.ds(start, HD), :])
        total = total + jnp.dot(
            jnp.concatenate(lhs, axis=1), jnp.concatenate(rhs, axis=0), preferred_element_type=f32
        )
    return total, square


def own_kernel(first_ref, pieces_ref, weight_far, total_ref, square_ref, weight_ref, sem):
    copy = pltpu.make_async_copy(weight_far, weight_ref, sem)
    copy.start()
    copy.wait()
    total_ref[...], square_ref[...] = share_of(pieces_ref, first_ref[0], weight_ref)


def last_kernel(first_ref, pieces_ref, weight_ref, total_ref, square_ref, out_ref, spread):
    rows = pieces_ref.shape[1]
    seqs = rows // PROP
    total, square = share_of(pieces_ref, 1 - first_ref[0], weight_ref)
    square = jnp.sum(square + square_ref[...], axis=1, keepdims=True)
    mixed = (total + total_ref[...]) * lax.rsqrt(square / (HG * G * HD) + 1e-05)
    for j in range(PROP):
        spread[:, j, :] = mixed[j * seqs : (j + 1) * seqs]
    out_ref[...] = spread[...].astype(jnp.bfloat16)


def pack(rows, copies):
    seqs = rows.shape[0]
    return pl.pallas_call(
        pack_kernel,
        out_shape=jax.ShapeDtypeStruct((copies, 2 * seqs, 2 * HD), jnp.bfloat16),
        in_specs=vmem(1),
        out_specs=vmem(1)[0],
        scratch_shapes=[pltpu.VMEM((PROP, seqs, HD), jnp.float32)],
        compiler_params=pltpu.CompilerParams(vmem_limit_bytes=8 << 20),
        interpret=INTERPRET,
        name="pack",
    )(rows)


def prep(*inputs):
    state = inputs[-1]
    seqs = state.shape[0]
    return pl.pallas_call(
        prep_kernel,
        out_shape=pltpu.VMEM((places(seqs)["end"], N), jnp.bfloat16),
        in_specs=[pl.BlockSpec(memory_space=pltpu.HBM)] * len(inputs),
        out_specs=vmem(1)[0],
        scratch_shapes=[pltpu.VMEM(x.shape, x.dtype) for x in inputs]
        + [pltpu.SemaphoreType.DMA((len(inputs),))],
        compiler_params=pltpu.CompilerParams(vmem_limit_bytes=16 << 20),
        cost_estimate=pl.CostEstimate(flops=1 << 24, bytes_accessed=4 << 20, transcendentals=0),
        interpret=INTERPRET,
        name="prep",
    )(*(in_hbm(x) for x in inputs))


def mixer(pieces, *rest):
    half = pieces.shape[2]
    return pl.pallas_call(
        mixer_kernel,
        out_shape=jax.ShapeDtypeStruct((2 * half, 2 * HD), jnp.bfloat16),
        in_specs=vmem(2) + hbm(3) + vmem(1),
        out_specs=vmem(1)[0],
        scratch_shapes=[
            pltpu.VMEM((half // 2, 2 * PROP, N), jnp.float32),
            pltpu.VMEM((half // 2, 2 * PROP, 2 * HD), jnp.float32),
            *(pltpu.VMEM(x.shape, x.dtype) for x in (rest[3], rest[2], rest[1])),
            pltpu.SemaphoreType.DMA((3,)),
        ],
        compiler_params=pltpu.CompilerParams(vmem_limit_bytes=20 << 20),
        cost_estimate=pl.CostEstimate(
            flops=2 * 2 * half * D * 5 * N, bytes_accessed=5 << 20, transcendentals=2 * half * 1000
        ),
        interpret=INTERPRET,
        name="mixer",
    )(pieces, *rest)


def cost_of(pieces, weight):
    kv_count, rows, width = pieces.shape
    return pl.CostEstimate(
        flops=2 * rows * kv_count * width * weight.shape[1], bytes_accessed=1 << 20, transcendentals=rows
    )


def own_half(first, pieces, weight):
    rows = pieces.shape[1]
    return pl.pallas_call(
        own_kernel,
        out_shape=[
            jax.ShapeDtypeStruct((rows, weight.shape[1]), jnp.float32),
            jax.ShapeDtypeStruct((rows, 2 * HD), jnp.float32),
            pltpu.VMEM(weight.shape, weight.dtype),
        ],
        in_specs=[pl.BlockSpec(memory_space=pltpu.SMEM)] + vmem(1) + hbm(1),
        out_specs=vmem(3),
        scratch_shapes=[pltpu.SemaphoreType.DMA],
        compiler_params=pltpu.CompilerParams(vmem_limit_bytes=16 << 20),
        cost_estimate=cost_of(pieces, weight),
        interpret=INTERPRET,
        name="own_half",
    )(first, pieces, in_hbm(weight))


def last(first, pieces, weight, total, square):
    rows = pieces.shape[1]
    seqs = rows // PROP
    cols = weight.shape[1]
    return pl.pallas_call(
        last_kernel,
        out_shape=jax.ShapeDtypeStruct((seqs, PROP, cols), jnp.bfloat16),
        in_specs=[pl.BlockSpec(memory_space=pltpu.SMEM)] + vmem(4),
        out_specs=vmem(1)[0],
        scratch_shapes=[pltpu.VMEM((seqs, PROP, cols), jnp.float32)],
        compiler_params=pltpu.CompilerParams(vmem_limit_bytes=16 << 20),
        cost_estimate=cost_of(pieces, weight),
        interpret=INTERPRET,
        name="last",
    )(first, pieces, weight, total, square)


def prepared(
    kv_index,
    tp_index,
    leading_scaling_factor,
    lane_feed_matrix,
    final_valve_matrix,
    increment_matrix,
    entry_basis_matrix,
    readout_basis_matrix,
    lane_feed_kernel,
    entry_basis_kernel,
    readout_basis_kernel,
    increment_offset,
    shrink_speed_exponent,
    lane_bypass_factor,
    hidden_carried_memory,
    lane_filter_memory,
    entry_basis_memory,
    readout_basis_memory,
    predecessor_index,
    admitted_counts,
    surplus_fading,
):
    seqs = predecessor_index.shape[0]
    heads = increment_offset.shape[0]
    wx = jnp.transpose(lane_feed_matrix, (1, 2, 3, 0)).reshape(heads * HD, D)
    wz = jnp.transpose(final_valve_matrix, (1, 2, 3, 0)).reshape(heads * HD, D)
    dt_own = lax.dynamic_slice(
        jnp.transpose(increment_matrix, (1, 2, 0)), (kv_index * heads, tp_index, 0), (heads, 1, D)
    )
    wb = entry_basis_matrix.reshape(D, N)
    wc = readout_basis_matrix.reshape(D, N)
    head_rows = jnp.stack(
        [x.reshape(heads) for x in (increment_offset, shrink_speed_exponent, lane_bypass_factor)]
    )
    tables = prep(
        leading_scaling_factor.reshape(1, D),
        dt_own.reshape(heads, D),
        jnp.transpose(lane_filter_memory, (1, 0, 2, 3, 4)).reshape(WIN, seqs, heads * HD),
        jnp.transpose(entry_basis_memory, (1, 0, 2, 3)).reshape(WIN, seqs, N),
        jnp.transpose(readout_basis_memory, (1, 0, 2, 3)).reshape(WIN, seqs, N),
        lane_feed_kernel,
        entry_basis_kernel,
        readout_basis_kernel,
        head_rows,
        jnp.transpose(predecessor_index),
        admitted_counts.reshape(1, seqs),
        jnp.transpose(surplus_fading, (1, 2, 3, 0)),
        hidden_carried_memory.reshape(seqs, heads * HD, N),
    )
    return (wx, in_hbm(wz), in_hbm(wb), in_hbm(wc), in_vmem(tables))


def shards(candidate_vectors, leading_scaling_factor, lane_feed_matrix, final_valve_matrix,
           increment_matrix, entry_basis_matrix, readout_basis_matrix, lane_feed_kernel,
           entry_basis_kernel, readout_basis_kernel, increment_offset, shrink_speed_exponent,
           lane_bypass_factor, final_linear_matrix, *memories):
    copies = pack(candidate_vectors, lax.axis_size(KV))
    along = lax.all_to_all(copies, KV, split_axis=0, concat_axis=0, tiled=True)
    pieces = lax.all_gather(along, "tp")
    rest = prepared(
        lax.axis_index(KV), lax.axis_index("tp"), leading_scaling_factor, lane_feed_matrix,
        final_valve_matrix, increment_matrix, entry_basis_matrix, readout_basis_matrix,
        lane_feed_kernel, entry_basis_kernel, readout_basis_kernel, increment_offset,
        shrink_speed_exponent, lane_bypass_factor, *memories,
    )
    gated = mixer(pieces, *rest)
    rings = [[G * z + (z + t) % G for z in range(lax.axis_size(KV))] for t in range(G)]
    along = lax.all_gather(gated, (KV, "tp"), axis_index_groups=rings)
    swapped = lax.ppermute(along, "tp", [(0, 1), (1, 0)])
    weight = final_linear_matrix.reshape(HG * G * HD, -1)
    first = ((lax.axis_index(KV) + lax.axis_index("tp")) % G).reshape(1)
    total, square, held = own_half(first, along, weight)
    return last(first, swapped, in_vmem(held), total, square)


def solution(mesh):
    placed = (
        P(("grp", "dp"), None, ("kv", "tp")),
        P(),
        P(None, KV, "tp", None),
        P(None, KV, "tp", None),
        P(),
        P(None, "tp", None),
        P(None, "tp", None),
        P(None, KV, "tp", None),
        P(None, "tp", None),
        P(None, "tp", None),
        P(KV, "tp"),
        P(KV, "tp"),
        P(KV, "tp"),
        P(None, None, None, ("kv", "tp")),
        P(("grp", "dp"), KV, "tp", None, None),
        P(("grp", "dp"), None, KV, "tp", None),
        P(("grp", "dp"), None, "tp", None),
        P(("grp", "dp"), None, "tp", None),
        P(("grp", "dp"), None),
        P(("grp", "dp")),
        P(("grp", "dp"), None, KV, "tp"),
    )
    return jax.shard_map(
        shards,
        mesh=mesh,
        in_specs=placed,
        out_specs=P(("grp", "dp"), None, ("kv", "tp")),
        check_vma=False,
    )
```
